32 devices in a mesh: fs: 4 (over y, x), tp: 8 (over z, core).
Axes of the slice: x: 2, y: 2, z: 4, core: 2. Of those that a mesh axis runs over, the one named last changes fastest.
Arguments:
- normed_inputs: bfloat16 [4096, 4096], P('fs', 'tp'), may hold values from -6 to 6
- query_upstream: bfloat16 [4096, 4096], P('fs', 'tp'), may hold values from -0.125 to 0.125
- key_upstream: bfloat16 [4096, 1024], P('fs', 'tp'), may hold values from -0.09375 to 0.09375
- head_outputs: bfloat16 [4096, 4096], P('fs', 'tp'), may hold values from -6 to 6
- branch_upstream: bfloat16 [4096, 4096], P('fs', 'tp'), may hold values from -0.125 to 0.125
- query_master: float32 [4096, 4096], P('fs', 'tp'), may hold values from -0.09375 to 0.09375
- key_master: float32 [4096, 1024], P('fs', 'tp'), may hold values from -0.09375 to 0.09375
- branch_master: float32 [4096, 4096], P('fs', 'tp'), may hold values from -0.09375 to 0.09375
- query_basis: bfloat16 [4096, 128], replicated, may hold values from -0.09375 to 0.09375
- key_basis: bfloat16 [4096, 128], replicated, may hold values from -0.09375 to 0.09375
- branch_basis: bfloat16 [4096, 128], replicated, may hold values from -0.09375 to 0.09375
- query_first: float32 [128, 4096], P(None, 'tp'), may hold values from -0.75 to 0.75
- query_second: float32 [128, 4096], P(None, 'tp'), may hold values from 0.001 to 0.02
- key_first: float32 [128, 1024], P(None, 'tp'), may hold values from -0.75 to 0.75
- key_second: float32 [128, 1024], P(None, 'tp'), may hold values from 0.001 to 0.02
- branch_first: float32 [4096, 128], P('fs'), may hold values from -0.75 to 0.75
- branch_second: float32 [4096, 128], P('fs'), may hold values from 0.001 to 0.02
Outputs:
- query_step: float32 [4096, 4096], P('fs', 'tp')
- key_step: float32 [4096, 1024], P('fs', 'tp')
- branch_step: float32 [4096, 4096], P('fs', 'tp')
- query_updated: float32 [4096, 4096], P('fs', 'tp')
- key_updated: float32 [4096, 1024], P('fs', 'tp')
- branch_updated: float32 [4096, 4096], P('fs', 'tp')
- query_copy: bfloat16 [4096, 4096], P(None, 'tp')
- key_copy: bfloat16 [4096, 1024], P(None, 'tp')
- branch_copy: bfloat16 [4096, 4096], P(None, 'tp')
- query_first_new: float32 [128, 4096], P(None, 'tp')
- query_second_new: float32 [128, 4096], P(None, 'tp')
- key_first_new: float32 [128, 1024], P(None, 'tp')
- key_second_new: float32 [128, 1024], P(None, 'tp')
- branch_first_new: float32 [4096, 128], P('fs')
- branch_second_new: float32 [4096, 128], P('fs')
The draws below stay inside these ranges and needn't reach their ends.
All inputs are finite; a program needn't handle non-finite values.
Results may differ from the reference program's by a relative error of at most 0.001.
Values may be sent and summed in bfloat16 or wider, within the bound.
A program may use at most 128 MiB of HBM per device.

```python
import math
import jax
import jax.numpy as jnp
from jax import lax

D = 4096
RANK = 128
HW = 4096
KW = 1024
TOKENS = 4096


def strengthened(drawn, own_key, source, target, blocks, factor):
    def block_of(axis_at):
        return (jnp.arange(drawn.shape[axis_at]) // (drawn.shape[axis_at] // blocks)).reshape((-1,) + (1,) * (drawn.ndim - 1 - axis_at))

    near = jax.random.permutation(own_key, blocks)[block_of(target)]
    other_side = (block_of(target) + blocks // 2) % blocks
    return jnp.where((block_of(source) == near) | (block_of(source) == other_side), factor * drawn, drawn)


def steps_of(key, extent, split, least, top_value):
    def one(position, blocks):
        draws = jax.random.uniform(jax.random.fold_in(jax.random.fold_in(key, 6), position), (blocks,), jnp.float32, least / len(split), top_value / len(split))
        return jnp.repeat(jnp.exp(draws), extent[position] // blocks).reshape((-1,) + (1,) * (len(extent) - position - 1))

    loudness = one(*split[0])
    for cut in split[1:]:
        loudness = loudness * one(*cut)
    return loudness


def centred(rng, extent, width, most, cuts=(), held_as=jnp.bfloat16):
    values = width * jax.random.normal(rng, extent, jnp.float32)
    if cuts:
        values = values * steps_of(rng, extent, cuts, -0.22, 0.18)
    return jnp.clip(values, -most, most).astype(held_as)


def gaussian_with(stream_key, dims, spread, limit, shards, heavy, kind=jnp.bfloat16):
    drawn = spread * jax.random.normal(stream_key, dims, jnp.float32)
    if shards:
        drawn = drawn * steps_of(stream_key, dims, shards, -0.22, 0.18)
    return jnp.clip(strengthened(drawn, jax.random.fold_in(stream_key, 3), *heavy), -limit, limit).astype(kind)


def setup_inputs(seed: int = 0) -> dict:
    key_list = jax.random.split(jax.random.key(seed), 18)
    normed_inputs = centred(key_list[0], (TOKENS, D), 1.0, 6.0, ((0, 4), (1, 8)))
    query_upstream = gaussian_with(key_list[1], (TOKENS, HW), TOKENS ** -0.5, 0.125, ((0, 4), (1, 8)), (0, 1, 8, 2.0))
    key_upstream = centred(key_list[2], (TOKENS, KW), TOKENS ** -0.5, 0.09375, ((0, 4), (1, 8)))
    head_outputs = centred(key_list[3], (TOKENS, HW), 1.0, 6.0, ((0, 4), (1, 8)))
    branch_upstream = gaussian_with(key_list[4], (TOKENS, D), TOKENS ** -0.5, 0.125, ((0, 4), (1, 8)), (0, 1, 8, 2.0))
    query_master = centred(key_list[5], (D, HW), D ** -0.5, 0.09375, ((0, 4), (1, 8)), jnp.float32)
    key_master = centred(key_list[6], (D, KW), D ** -0.5, 0.09375, ((0, 4), (1, 8)), jnp.float32)
    branch_master = centred(key_list[7], (HW, D), HW ** -0.5, 0.09375, ((0, 4), (1, 8)), jnp.float32)
    query_basis = centred(key_list[8], (D, RANK), D ** -0.5, 0.09375)
    key_basis = centred(key_list[9], (D, RANK), D ** -0.5, 0.09375)
    branch_basis = centred(key_list[10], (D, RANK), D ** -0.5, 0.09375)
    query_first = centred(key_list[11], (RANK, HW), 0.05, 0.75, ((1, 8),), jnp.float32)
    query_second = jnp.clip(jnp.exp(math.log(0.02) - 2.9957322 * jax.random.uniform(key_list[12], (RANK, HW), jnp.float32) ** steps_of(key_list[12], (RANK, HW), ((1, 8),), -0.2, 0.2)), 0.001, 0.02)
    key_first = centred(key_list[13], (RANK, KW), 0.05, 0.75, ((1, 8),), jnp.float32)
    key_second = jnp.clip(jnp.exp(math.log(0.02) - 2.9957322 * jax.random.uniform(key_list[14], (RANK, KW), jnp.float32) ** steps_of(key_list[14], (RANK, KW), ((1, 8),), -0.2, 0.2)), 0.001, 0.02)
    branch_first = centred(key_list[15], (HW, RANK), 0.05, 0.75, ((0, 4),), jnp.float32)
    branch_second = jnp.clip(jnp.exp(math.log(0.02) - 2.9957322 * jax.random.uniform(key_list[16], (HW, RANK), jnp.float32) ** steps_of(key_list[16], (HW, RANK), ((0, 4),), -0.2, 0.2)), 0.001, 0.02)
    return {"normed_inputs": normed_inputs, "query_upstream": query_upstream, "key_upstream": key_upstream, "head_outputs": head_outputs, "branch_upstream": branch_upstream, "query_master": query_master, "key_master": key_master, "branch_master": branch_master, "query_basis": query_basis, "key_basis": key_basis, "branch_basis": branch_basis, "query_first": query_first, "query_second": query_second, "key_first": key_first, "key_second": key_second, "branch_first": branch_first, "branch_second": branch_second}


LEARN = 0.02
BETA_ONE = 0.9
BETA_TWO = 0.95
ADAM_EPS = 1e-08
CLIP_RMS = 0.5

def moments(first, second, low, clip):
    scaled = clip * low
    first_new = BETA_ONE * first + (1.0 - BETA_ONE) * scaled
    second_new = BETA_TWO * second + (1.0 - BETA_TWO) * scaled * scaled
    return (first_new, second_new, first_new / (jnp.sqrt(second_new) + ADAM_EPS))

def reference(normed_inputs, query_upstream, key_upstream, head_outputs, branch_upstream, query_master, key_master, branch_master, query_basis, key_basis, branch_basis, query_first, query_second, key_first, key_second, branch_first, branch_second):
    exact = lax.Precision.HIGHEST
    query_grad = jnp.dot(normed_inputs.T, query_upstream, preferred_element_type=jnp.float32)
    key_grad = jnp.dot(normed_inputs.T, key_upstream, preferred_element_type=jnp.float32)
    branch_grad = jnp.dot(head_outputs.T, branch_upstream, preferred_element_type=jnp.float32)
    query_low = jnp.dot(query_basis.astype(jnp.float32).T, query_grad, precision=exact)
    key_low = jnp.dot(key_basis.astype(jnp.float32).T, key_grad, precision=exact)
    branch_low = jnp.dot(branch_grad, branch_basis.astype(jnp.float32), precision=exact)
    total = jnp.sum(query_low * query_low) + jnp.sum(key_low * key_low) + jnp.sum(branch_low * branch_low)
    entries = query_low.size + key_low.size + branch_low.size
    rms_value = jnp.sqrt(total / float(entries))
    clip = 1.0 / jnp.maximum(1.0, rms_value / CLIP_RMS)
    q_first, q_second, q_dir = moments(query_first, query_second, query_low, clip)
    k_first, k_second, k_dir = moments(key_first, key_second, key_low, clip)
    b_first, b_second, b_dir = moments(branch_first, branch_second, branch_low, clip)
    query_step = jnp.dot(query_basis.astype(jnp.float32), q_dir, precision=exact)
    key_step = jnp.dot(key_basis.astype(jnp.float32), k_dir, precision=exact)
    branch_step = jnp.dot(b_dir, branch_basis.astype(jnp.float32).T, precision=exact)
    query_updated = query_master - LEARN * query_step
    key_updated = key_master - LEARN * key_step
    branch_updated = branch_master - LEARN * branch_step
    return (query_step, key_step, branch_step, query_updated, key_updated, branch_updated, query_updated.astype(jnp.bfloat16), key_updated.astype(jnp.bfloat16), branch_updated.astype(jnp.bfloat16), q_first, q_second, k_first, k_second, b_first, b_second)
```

```python
import functools

import jax
import jax.numpy as jnp
from jax import lax
from jax.experimental import pallas as pl
from jax.experimental.pallas import tpu as pltpu
from jax.sharding import PartitionSpec as P

LEARN = 0.02
BETA_ONE = 0.9
BETA_TWO = 0.95
ADAM_EPS = 1e-08
CLIP_RMS = 0.5


def moments(first, second, low, clip):
    scaled = clip * low
    first_new = BETA_ONE * first + (1.0 - BETA_ONE) * scaled
    second_new = BETA_TWO * second + (1.0 - BETA_TWO) * scaled * scaled
    return (first_new, second_new, first_new / (jnp.sqrt(second_new) + ADAM_EPS))


def over_tokens(left, right, precision=None):
    return lax.dot_general(
        left,
        right,
        (((0,), (0,)), ((), ())),
        precision=precision,
        preferred_element_type=jnp.float32,
    )


def split_three(values):
    high = values.astype(jnp.bfloat16)
    rest = values - high.astype(jnp.float32)
    middle = rest.astype(jnp.bfloat16)
    low = (rest - middle.astype(jnp.float32)).astype(jnp.bfloat16)
    return high, middle, low


class Sender:
    def __init__(self, send_sem, recv_sem):
        self.send_sem, self.recv_sem, self.used, self.started = send_sem, recv_sem, 0, []

    def reserve(self, count):
        self.used += count
        return self.used - count

    def start(self, source, target, device):
        copy = pltpu.make_async_remote_copy(
            src_ref=source,
            dst_ref=target,
            send_sem=self.send_sem.at[self.used],
            recv_sem=self.recv_sem.at[self.used],
            device_id=device,
            device_id_type=pl.DeviceIdType.MESH,
        )
        self.used += 1
        copy.start()
        self.started.append(copy)
        return copy

    def drain(self):
        for copy in self.started:
            copy.wait_send()


def greet(nf, nt, row, col, both):
    barrier = pltpu.get_barrier_semaphore()
    peers = [{"fs": lax.rem(row + o, nf), "tp": col} for o in range(1, nf)]
    if both:
        peers += [{"fs": row, "tp": lax.rem(col + o, nt)} for o in range(1, nt)]
    for peer in peers:
        pl.semaphore_signal(
            barrier, inc=1, device_id=peer, device_id_type=pl.DeviceIdType.MESH
        )
    pl.semaphore_wait(barrier, len(peers))


def square(row, col):
    side = row + 1 - 2 * lax.rem(row, 2)
    front = lax.rem(row + 2, 4)
    return side, front, ({"fs": side, "tp": col}, {"fs": front, "tp": col})


def reduce_kernel(
    nf, nt,
    x_hbm, qu_hbm, ku_hbm, h_hbm, bu_hbm, master_ref, qb_ref, kb_ref, bb_ref,
    qk_out, b_out, total_out, far_out,
    x_ref, qu_ref, ku_ref, h_ref, bu_ref,
    part, from_pair, halves, arrived, whole, other,
    part_qk, part_b, got_qk, got_b, all_qk, all_b, spread_b, sums,
    send_sem, recv_sem, load_sem,
):
    row, col = lax.axis_index("fs"), lax.axis_index("tp")
    core, height = lax.rem(col, 2), lax.div(col, 2)
    nz = nt // 2
    rank = qb_ref.shape[1]
    half = x_ref.shape[0] // 2
    piece = half // nz
    query_cols = qu_ref.shape[1]
    loads = []

    def load(source, target):
        copy = pltpu.make_async_copy(source, target, load_sem.at[len(loads)])
        copy.start()
        loads.append(copy)

    for which in (1 - core, core):
        rows = pl.ds(pl.multiple_of(which * half, half), half)
        load(x_hbm.at[rows], x_ref.at[rows])
        load(bu_hbm.at[rows], bu_ref.at[rows])
    load(qu_hbm, qu_ref)
    load(ku_hbm, ku_ref)
    load(h_hbm, h_ref)
    greet(nf, nt, row, col, True)
    sender = Sender(send_sem, recv_sem)
    pair = {"fs": row, "tp": height * 2 + (1 - core)}

    def above(o):
        return {"fs": row, "tp": lax.rem(height + o, nz) * 2 + core}

    def beside(o):
        return {"fs": lax.rem(row + o, nf), "tp": col}

    def project(which):
        rows = pl.ds(pl.multiple_of(which * half, half), half)
        x = x_ref[rows, :]
        return (
            jnp.dot(x, qb_ref[...], preferred_element_type=jnp.float32),
            jnp.dot(x, kb_ref[...], preferred_element_type=jnp.float32),
            jnp.dot(bu_ref[rows, :], bb_ref[...], preferred_element_type=jnp.float32),
        )

    early = far_out.shape[1]
    sent = []
    if nf == 4:
        side, front, names = square(row, col)
        for turn in range(2):
            for n in range(2):
                rows = pl.ds((turn ^ n) * (early // 2), early // 2)
                sent.append(
                    sender.start(master_ref.at[rows], far_out.at[row, rows], names[n])
                )
    else:
        rows = pl.ds(0, early)
        for o in range(1, nf):
            sent.append(sender.start(master_ref.at[rows], far_out.at[row], beside(o)))
    loads[0].wait()
    loads[1].wait()
    for n, value in enumerate(project(1 - core)):
        part[:, n * rank : (n + 1) * rank] = value
    swap = sender.start(part, from_pair, pair)
    loads[2].wait()
    loads[3].wait()
    own = project(core)
    swap.wait_recv()
    for n, value in enumerate(own):
        span = slice(n * rank, (n + 1) * rank)
        halves[:, :, span] = (value + from_pair[:, span]).reshape(nz, piece, rank)
    copies = [
        sender.start(halves.at[lax.rem(height + o, nz)], arrived.at[o - 1], above(o))
        for o in range(1, nz)
    ]
    total = halves[height]
    for o, copy in enumerate(copies):
        copy.wait_recv()
        total = total + arrived[o]
    whole[height] = total
    copies = [sender.start(whole.at[height], whole.at[height], above(o)) for o in range(1, nz)]
    across = [sender.start(whole.at[height], other.at[height], pair)]
    passed = []
    if nf == 4:
        for n, source in ((0, side), (1, front)):
            sent[n].wait_recv()
            held = far_out.at[source, pl.ds(n * (early // 2), early // 2)]
            passed.append(sender.start(held, held, names[1 - n]))
    for o, copy in enumerate(copies, 1):
        copy.wait_recv()
        source = lax.rem(height + nz - o, nz)
        across.append(sender.start(whole.at[source], other.at[source], pair))

    over_rows = (((0,), (0,)), ((), ()))

    def low_parts(values, which):
        rows = pl.ds(pl.multiple_of(which * half, half), half)
        sides = (qu_ref[rows, :], ku_ref[rows, :], h_ref[rows, :])
        parts = []
        for n, side in enumerate(sides):
            terms = split_three(values[:, n * rank : (n + 1) * rank])
            parts.append(
                sum(
                    lax.dot_general(term, side, over_rows, preferred_element_type=jnp.float32)
                    for term in terms
                )
            )
        return parts

    for copy in loads[4:]:
        copy.wait()
    first = low_parts(whole[...].reshape(half, 3 * rank), core)
    for copy in across:
        copy.wait_recv()
    second = low_parts(other[...].reshape(half, 3 * rank), 1 - core)
    query_part, key_part, branch_part = [a + b for a, b in zip(first, second)]
    part_qk[:, :, :query_cols] = query_part.reshape(nf, rank // nf, query_cols)
    part_qk[:, :, query_cols:] = key_part.reshape(nf, rank // nf, key_part.shape[1])
    part_b[...] = branch_part.T.reshape(part_b.shape)

    copies = []
    for o in range(1, nf):
        to = lax.rem(row + o, nf)
        copies.append(sender.start(part_qk.at[to], got_qk.at[o - 1], beside(o)))
        copies.append(sender.start(part_b.at[to], got_b.at[o - 1], beside(o)))
    for copy in copies:
        copy.wait_recv()
    sum_qk, sum_b = part_qk[row], part_b[row]
    for o in range(nf - 1):
        sum_qk = sum_qk + got_qk[o]
        sum_b = sum_b + got_b[o]
    rows_b = sum_b.shape[0]
    squares = jnp.sum(sum_qk * sum_qk) + jnp.sum(sum_b * sum_b)
    all_qk[row] = sum_qk
    all_b[col, :rows_b, :] = sum_b
    all_b[col, rows_b:, :] = jnp.full((8, rank), squares, jnp.float32)

    copies_b = [
        sender.start(all_b.at[col], all_b.at[col], {"fs": row, "tp": lax.rem(col + o, nt)})
        for o in range(1, nt)
    ]
    copies_qk = [sender.start(all_qk.at[row], all_qk.at[row], beside(o)) for o in range(1, nf)]
    for copy in copies_b:
        copy.wait_recv()
    sums[row] = jnp.sum(all_b[:, rows_b:, :], axis=0)
    each = nt // nf
    copies = []
    for o in range(1, nf):
        blocks = pl.ds(lax.rem(row + o, nf) * each, each)
        copies.append(sender.start(sums.at[row], sums.at[row], beside(o)))
        copies.append(sender.start(all_b.at[blocks], spread_b.at[row], beside(o)))
    b_out[:, row] = all_b[pl.ds(row * each, each)][:, :rows_b, :]
    for copy in copies_qk:
        copy.wait_recv()
    qk_out[...] = all_qk[...].reshape(qk_out.shape)
    for copy in copies:
        copy.wait_recv()
    for o in range(1, nf):
        source = lax.rem(row + o, nf)
        b_out[:, source] = spread_b[source][:, :rows_b, :]
    total_out[...] = jnp.sum(sums[...], axis=0)
    for copy in (sent[2:] + passed) if nf == 4 else sent:
        copy.wait_recv()
    sender.drain()


def reduced(nf, nt, early, x, qu, ku, h, bu, master, qb, kb, bb):
    tokens, features = x.shape
    rank = qb.shape[1]
    cols = qu.shape[1] + ku.shape[1]
    half, nz, each = tokens // 2, nt // 2, nt // nf
    piece, thin, rows_b = half // nz, rank // nf, features // nf
    copies = 1 + 2 * (nz - 1) + nz + 2 * (nf - 1) + (nt - 1) + 3 * (nf - 1)
    copies += 6 if nf == 4 else nf - 1
    any_place = pl.BlockSpec(memory_space=pl.ANY)
    vmem = pl.BlockSpec(memory_space=pltpu.VMEM)
    f32 = jnp.float32
    return pl.pallas_call(
        functools.partial(reduce_kernel, nf, nt),
        out_shape=(
            jax.ShapeDtypeStruct((rank, cols), f32),
            jax.ShapeDtypeStruct((each, nf, rows_b, rank), f32),
            jax.ShapeDtypeStruct((8, rank), f32),
            jax.ShapeDtypeStruct((nf, early, master.shape[1]), f32),
        ),
        in_specs=[any_place] * 6 + [vmem] * 3,
        out_specs=(vmem, vmem, vmem, any_place),
        scratch_shapes=[
            *[pltpu.VMEM(each_in.shape, each_in.dtype) for each_in in (x, qu, ku, h, bu)],
            pltpu.VMEM((half, 3 * rank), f32),
            pltpu.VMEM((half, 3 * rank), f32),
            pltpu.VMEM((nz, piece, 3 * rank), f32),
            pltpu.VMEM((nz - 1, piece, 3 * rank), f32),
            pltpu.VMEM((nz, piece, 3 * rank), f32),
            pltpu.VMEM((nz, piece, 3 * rank), f32),
            pltpu.VMEM((nf, thin, cols), f32),
            pltpu.VMEM((nf, rows_b, rank), f32),
            pltpu.VMEM((nf - 1, thin, cols), f32),
            pltpu.VMEM((nf - 1, rows_b, rank), f32),
            pltpu.VMEM((nf, thin, cols), f32),
            pltpu.VMEM((nt, rows_b + 8, rank), f32),
            pltpu.VMEM((nf, each, rows_b + 8, rank), f32),
            pltpu.VMEM((nf, 8, rank), f32),
            pltpu.SemaphoreType.DMA((copies,)),
            pltpu.SemaphoreType.DMA((copies,)),
            pltpu.SemaphoreType.DMA((7,)),
        ],
        compiler_params=pltpu.CompilerParams(
            collective_id=0, has_side_effects=True, vmem_limit_bytes=58 * 2**20
        ),
    )(x, qu, ku, h, bu, master, qb, kb, bb)


def gather_kernel(
    nf, nt,
    q_ref, b_ref, k_ref, far_ref, master_ref, basis_ref, dir_ref,
    q_out, b_out, k_out,
    held_far, held_copy, send_sem, recv_sem, own_sem, load_sem, store_sem,
):
    row, col = lax.axis_index("fs"), lax.axis_index("tp")
    early = far_ref.shape[1]
    pairs = ((q_ref, q_out, early), (b_ref, b_out, 0), (k_ref, k_out, 0))

    def load(o):
        source = master_ref.at[pl.ds(0, early)] if o == 0 else far_ref.at[lax.rem(row + o, nf)]
        copy = pltpu.make_async_copy(source, held_far.at[o % 2], load_sem.at[o])
        copy.start()
        return copy

    coming = load(0)
    greet(nf, nt, row, col, False)
    sender = Sender(send_sem, recv_sem)
    sent = []
    if nf == 4:
        side, front, names = square(row, col)
        for ref, out, base in pairs:
            half = ref.shape[0] // 2
            for h in range(2):
                rows = pl.ds(h * half, half)
                target = pl.ds(base + h * half, half)
                for n in ((0, 1), (1, 0))[h]:
                    copy = sender.start(ref.at[rows], out.at[row, target], names[n])
                    sent.append((n, h, out, target, copy))
    else:
        for ref, out, base in pairs:
            for o in range(1, nf):
                target = out.at[row, pl.ds(base, ref.shape[0])]
                there = {"fs": lax.rem(row + o, nf), "tp": col}
                sent.append(sender.start(ref, target, there))
    local = []
    for n, (ref, out, base) in enumerate(pairs):
        target = out.at[row, pl.ds(base, ref.shape[0])]
        local.append(pltpu.make_async_copy(ref, target, own_sem.at[n]))
        local[-1].start()

    terms = split_three(dir_ref[...])
    rows_all = q_out.shape[1]
    stores = []
    for o in range(nf):
        source = lax.rem(row + o, nf)
        coming.wait()
        if o + 1 < nf:
            coming = load(o + 1)
        if o >= 2:
            stores[o - 2].wait()
        basis = basis_ref[pl.ds(pl.multiple_of(source * rows_all, rows_all), early), :]
        step = sum(jnp.dot(basis, term, preferred_element_type=jnp.float32) for term in terms)
        held_copy[o % 2] = (held_far[o % 2] - LEARN * step).astype(held_copy.dtype)
        stores.append(
            pltpu.make_async_copy(
                held_copy.at[o % 2], q_out.at[source, pl.ds(0, early)], store_sem.at[o]
            )
        )
        stores[-1].start()

    if nf == 4:
        last = []
        for n, h, out, target, copy in sent:
            copy.wait_recv()
            if n == h:
                held = out.at[(side, front)[n], target]
                last.append(sender.start(held, held, names[1 - n]))
        sent = last
    for copy in sent:
        copy.wait_recv()
    for copy in local + stores[-2:]:
        copy.wait()
    sender.drain()


def gathered_rows(nf, nt, q_tail, b_block, k_block, far, master, basis, direction):
    count = 18 if nf == 4 else 3 * (nf - 1)
    early = far.shape[1]
    blocks = (master, b_block, k_block)
    wide = [jax.ShapeDtypeStruct((nf, *block.shape), q_tail.dtype) for block in blocks]
    vmem = pl.BlockSpec(memory_space=pltpu.VMEM)
    any_place = pl.BlockSpec(memory_space=pl.ANY)
    outs = pl.pallas_call(
        functools.partial(gather_kernel, nf, nt),
        out_shape=tuple(wide),
        in_specs=[vmem] * 3 + [any_place] * 2 + [vmem] * 2,
        out_specs=(any_place,) * 3,
        scratch_shapes=[
            pltpu.VMEM((2, early, far.shape[2]), far.dtype),
            pltpu.VMEM((2, early, far.shape[2]), q_tail.dtype),
            pltpu.SemaphoreType.DMA((count,)),
            pltpu.SemaphoreType.DMA((count,)),
            pltpu.SemaphoreType.DMA((3,)),
            pltpu.SemaphoreType.DMA((nf,)),
            pltpu.SemaphoreType.DMA((nf,)),
        ],
        compiler_params=pltpu.CompilerParams(
            collective_id=1, has_side_effects=True, vmem_limit_bytes=48 * 2**20
        ),
    )(q_tail, b_block, k_block, far, master, basis, direction)
    return [out.reshape(-1, out.shape[-1]) for out in outs]


EARLY_OF_64 = 56
VMEM_LIMIT = 40 * 2**20
MASTER_MOST = 0.09375
MASTER_POWER = 14
MASTER_GAIN = 515.0 / MASTER_MOST
SUM_POWER = 16
SUM_GAIN = 238.0


def raised(magnitude, power):
    result, square = None, magnitude
    while power:
        if power % 2:
            result = square if result is None else result * square
        power //= 2
        if power:
            square = square * square
    return result


def coded(values, power):
    high = raised(jnp.abs(values), power)
    return jnp.where(values < 0, -high, high).astype(jnp.bfloat16)


def decoded(codes, power):
    codes = codes.astype(jnp.float32)
    root = jnp.exp(jnp.log(jnp.abs(codes)) * (1.0 / power))
    root = jnp.where(codes == 0, 0.0, root)
    return jnp.where(codes < 0, -root, root)


def column_scale(values):
    most = jnp.max(jnp.abs(values), axis=0, keepdims=True)
    return jnp.maximum(most, 1e-30).astype(jnp.bfloat16)


def pack_columns(values):
    scale = column_scale(values)
    codes = coded(values * (SUM_GAIN / scale.astype(jnp.float32)), SUM_POWER)
    return codes, jnp.broadcast_to(scale, (16, values.shape[1]))


def unpack_columns(codes, scale):
    return decoded(codes, SUM_POWER) * (scale[0:1].astype(jnp.float32) * (1.0 / SUM_GAIN))


def split_two(values):
    high = values.astype(jnp.bfloat16)
    return high, (values - high.astype(jnp.float32)).astype(jnp.bfloat16)


def exact_dot(left, terms):
    return sum(jnp.dot(left, term, preferred_element_type=jnp.float32) for term in terms)


def fused_kernel(
    nf, nt, early,
    x_hbm, qu_hbm, ku_hbm, h_hbm, bu_hbm, mq_hbm, mk_hbm, mb_hbm, qb_hbm, kb_hbm, bb_hbm,
    qf_hbm, qs_hbm, kf_hbm, ks_hbm, bf_hbm, bs_hbm,
    q_step, k_step, b_step, q_new, k_new, b_new, q_out, k_out, b_out,
    qf_out, qs_out, kf_out, ks_out, bf_out, bs_out,
    x_ref, qu_ref, ku_ref, h_ref, bu_ref, mq_ref, mk_ref, mb_ref, qb_ref, kb_ref,
    qf_ref, qs_ref, kf_ref, ks_ref, bf_ref, bs_ref, own_ref, turned, bbt_ref,
    part, from_pair, halves, sent_z, arrived, whole, other, split_ref,
    part_qk, part_b, got_qk, got_b, all_qk, own_b, blocks_b, pair_b, sums_f, sums_t,
    enc, far,
    send_sem, recv_sem, load_sem, b_recv,
):
    row, col = lax.axis_index("fs"), lax.axis_index("tp")
    core, height = lax.rem(col, 2), lax.div(col, 2)
    nz = nt // 2
    rank = qb_ref.shape[1]
    tokens, features = x_ref.shape
    half = tokens // 2
    piece = half // nz
    query_cols, key_cols = qu_ref.shape[1], ku_ref.shape[1]
    rows_in = mq_ref.shape[0]
    loads = {}

    def load(name, source, target):
        copy = pltpu.make_async_copy(source, target, load_sem.at[len(loads)])
        copy.start()
        loads[name] = copy

    def token_rows(which):
        return pl.ds(pl.multiple_of(which * half, half), half)

    first, second = pl.ds(0, early // 2), pl.ds(early // 2, early // 2)
    load("mq0", mq_hbm.at[first], mq_ref.at[first])
    load("mq1", mq_hbm.at[second], mq_ref.at[second])
    own_rows = pl.ds(pl.multiple_of(col * features, features), features)
    for n, basis in enumerate((qb_hbm, kb_hbm, bb_hbm)):
        load(("own", n), basis.at[own_rows], own_ref.at[n])
    for n, which in enumerate((1 - core, core)):
        load(("x", n), x_hbm.at[token_rows(which)], x_ref.at[token_rows(which)])
        load(("bu", n), bu_hbm.at[token_rows(which)], bu_ref.at[token_rows(which)])
    load("qu", qu_hbm, qu_ref)
    load("ku", ku_hbm, ku_ref)
    load("h", h_hbm, h_ref)
    if early < rows_in:
        rest = pl.ds(early, rows_in - early)
        load("mq2", mq_hbm.at[rest], mq_ref.at[rest])
    for name, source, target in (
        ("qf", qf_hbm, qf_ref), ("qs", qs_hbm, qs_ref), ("kf", kf_hbm, kf_ref), ("ks", ks_hbm, ks_ref),
        ("qb", qb_hbm, qb_ref), ("kb", kb_hbm, kb_ref), ("mk", mk_hbm, mk_ref),
        ("bf", bf_hbm, bf_ref), ("bs", bs_hbm, bs_ref), ("mb", mb_hbm, mb_ref),
    ):
        load(name, source, target)

    greet(nf, nt, row, col, True)
    sender = Sender(send_sem, recv_sem)
    pair = {"fs": row, "tp": height * 2 + (1 - core)}
    side, front, names = square(row, col)

    def above(o):
        return {"fs": row, "tp": lax.rem(height + o, nz) * 2 + core}

    def beside(o):
        return {"fs": lax.rem(row + o, nf), "tp": col}

    parts = (first, second)
    sent = []
    for turn in range(2):
        if turn == 0:
            for n in range(2):
                loads[f"mq{n}"].wait()
                enc[parts[n], :] = coded(mq_ref[parts[n], :] * MASTER_GAIN, MASTER_POWER)
        for n in range(2):
            rows = parts[turn ^ n]
            sent.append(sender.start(enc.at[rows], far.at[row, rows], names[n]))

    for n in range(3):
        loads["own", n].wait()
        turned[n * rank : (n + 1) * rank, :] = own_ref[n].T

    def project(n, which):
        loads["x", n].wait()
        loads["bu", n].wait()
        over = (((1,), (1,)), ((), ()))
        a = lax.dot_general(turned[: 2 * rank, :], x_ref[token_rows(which), :], over, preferred_element_type=jnp.float32)
        b = lax.dot_general(turned[2 * rank :, :], bu_ref[token_rows(which), :], over, preferred_element_type=jnp.float32)
        return a, b

    a, b = project(0, 1 - core)
    part[: 2 * rank, :] = a
    part[2 * rank :, :] = b
    swap = sender.start(part, from_pair, pair)
    a, b = project(1, core)
    swap.wait_recv()
    for n in range(nz):
        span = slice(n * piece, (n + 1) * piece)
        halves[n, : 2 * rank, :] = a[:, span] + from_pair[: 2 * rank, span]
        halves[n, 2 * rank :, :] = b[:, span] + from_pair[2 * rank :, span]

    def put(target, n, values):
        for k in range(3):
            codes, scale = pack_columns(values[k * rank : (k + 1) * rank])
            target[n, k * rank : (k + 1) * rank, :] = codes
            target[n, 3 * rank + 16 * k : 3 * rank + 16 * (k + 1), :] = scale

    def take(source, n, k):
        return unpack_columns(
            source[n, k * rank : (k + 1) * rank, :],
            source[n, 3 * rank + 16 * k : 3 * rank + 16 * (k + 1), :],
        )

    copies = []
    for o in range(1, nz):
        to = lax.rem(height + o, nz)
        put(sent_z, to, halves[to])
        copies.append(sender.start(sent_z.at[to], arrived.at[o - 1], above(o)))
    for copy in copies:
        copy.wait_recv()
    for k in range(3):
        span = slice(k * rank, (k + 1) * rank)
        total = halves[height, span, :]
        for o in range(nz - 1):
            total = total + take(arrived, o, k)
        codes, scale = pack_columns(total)
        whole[height, span, :] = codes
        whole[height, 3 * rank + 16 * k : 3 * rank + 16 * (k + 1), :] = scale
    copies = [sender.start(whole.at[height], whole.at[height], above(o)) for o in range(1, nz)]
    across = [sender.start(whole.at[height], other.at[height], pair)]

    passed = []
    for n, source in ((0, side), (1, front)):
        sent[n].wait_recv()
        held = far.at[source, parts[n]]
        passed.append(sender.start(held, held, names[1 - n]))

    bbt_ref[...] = turned[2 * rank :, :]
    for o, copy in enumerate(copies, 1):
        copy.wait_recv()
        source = lax.rem(height + nz - o, nz)
        across.append(sender.start(whole.at[source], other.at[source], pair))

    def low_parts(held, which):
        for n in range(nz):
            for k in range(3):
                high, low = split_two(take(held, n, k))
                split_ref[k, :rank, n * piece : (n + 1) * piece] = high
                split_ref[k, rank:, n * piece : (n + 1) * piece] = low
        lows = []
        for k, ref in enumerate((qu_ref, ku_ref, h_ref)):
            both = jnp.dot(split_ref[k], ref[token_rows(which), :], preferred_element_type=jnp.float32)
            lows.append(both[:rank] + both[rank:])
        return lows

    for name in ("qu", "ku", "h"):
        loads[name].wait()
    one = low_parts(whole, core)
    for copy in across:
        copy.wait_recv()
    two = low_parts(other, 1 - core)
    thin, wide = rank // nf, features // nf
    query_part, key_part, branch_part = [a + b for a, b in zip(one, two)]
    part_qk[:, :, :query_cols] = query_part.reshape(nf, thin, query_cols)
    part_qk[:, :, query_cols:] = key_part.reshape(nf, thin, key_cols)
    for n in range(nf):
        part_b[n] = branch_part[:, n * wide : (n + 1) * wide]

    copies = []
    for o in range(1, nf):
        to = lax.rem(row + o, nf)
        copies.append(sender.start(part_qk.at[to], got_qk.at[o - 1], beside(o)))
        copies.append(sender.start(part_b.at[to], got_b.at[o - 1], beside(o)))
    for copy in copies:
        copy.wait_recv()
    sum_qk, sum_b = part_qk[row], part_b[row]
    for o in range(nf - 1):
        sum_qk = sum_qk + got_qk[o]
        sum_b = sum_b + got_b[o]
    squares = jnp.sum(sum_qk * sum_qk) + jnp.sum(sum_b * sum_b)
    sums_f[row] = jnp.full((8, 128), squares, jnp.float32)
    copies_s = [sender.start(sums_f.at[row], sums_f.at[row], beside(o)) for o in range(1, nf)]
    all_qk[row] = sum_qk
    copies_qk = [sender.start(all_qk.at[row], all_qk.at[row], beside(o)) for o in range(1, nf)]
    sum_b = sum_b.T
    codes, scale = pack_columns(sum_b)
    own_b[:wide, :] = codes
    own_b[wide:, :] = scale

    spread = sender.reserve(nz - 1)
    to_owner = sender.reserve(1)
    owner = {"fs": height, "tp": col}

    def to_block(source, target):
        return pltpu.make_async_remote_copy(
            src_ref=source, dst_ref=target, send_sem=send_sem.at[to_owner], recv_sem=b_recv.at[row],
            device_id=owner, device_id_type=pl.DeviceIdType.MESH,
        )

    @pl.when(row != height)
    def _():
        to_block(own_b, blocks_b.at[row]).start()

    for copy in copies_s:
        copy.wait_recv()
    sums_t[col] = jnp.sum(sums_f[...], axis=0)
    copies_s = [
        sender.start(sums_t.at[col], sums_t.at[col], {"fs": row, "tp": lax.rem(col + o, nt)})
        for o in range(1, nt)
    ]

    def spread_copy(o):
        return pltpu.make_async_remote_copy(
            src_ref=blocks_b, dst_ref=blocks_b, send_sem=send_sem.at[spread + o - 1], recv_sem=b_recv.at[nf],
            device_id=above(o), device_id_type=pl.DeviceIdType.MESH,
        )

    @pl.when(row == height)
    def _():
        blocks_b[row] = own_b[...]
        for o in range(1, nf):
            source = lax.rem(row + o, nf)
            pltpu.make_async_remote_copy(
                src_ref=own_b, dst_ref=blocks_b.at[source], send_sem=send_sem.at[to_owner],
                recv_sem=b_recv.at[source], device_id=owner, device_id_type=pl.DeviceIdType.MESH,
            ).wait_recv()
        for o in range(1, nz):
            spread_copy(o).start()

    for copy in copies_qk:
        copy.wait_recv()
    for name in ("qf", "qs", "kf", "ks", "qb", "kb", "mk") + (("mq2",) if early < rows_in else ()):
        loads[name].wait()
    for copy in copies_s:
        copy.wait_recv()
    total = jnp.sum(sums_t[...], axis=0)[0:1, 0:1]
    entries = rank * nt * (2 * query_cols + key_cols)
    clip = 1.0 / jnp.maximum(1.0, jnp.sqrt(total / float(entries)) / CLIP_RMS)

    lows = all_qk[...].reshape(rank, query_cols + key_cols)
    qf_out[...], qs_out[...], q_dir = moments(qf_ref[...], qs_ref[...], lows[:, :query_cols], clip)
    kf_out[...], ks_out[...], k_dir = moments(kf_ref[...], ks_ref[...], lows[:, query_cols:], clip)
    q_terms, k_terms = split_two(q_dir), split_two(k_dir)
    late = []

    def send_block(out, base, count):
        part_rows = count // 2
        for h in range(2):
            target = pl.ds(base + h * part_rows, part_rows)
            for n in ((0, 1), (1, 0))[h]:
                held = out.at[row, target]
                late.append((n, h, out, target, sender.start(held, held, names[n])))

    def basis_rows(ref, source, base, count):
        return ref[pl.ds(pl.multiple_of(source * rows_in + base, 16), count), :]

    def own_update(step_ref, new_ref, out, master, basis, terms, base, count):
        rows = slice(base, base + count)
        step = exact_dot(basis_rows(basis, row, base, count), terms)
        step_ref[rows, :] = step
        updated = master[rows, :] - LEARN * step
        new_ref[rows, :] = updated
        out[row, rows, :] = updated.astype(out.dtype)

    if early < rows_in:
        own_update(q_step, q_new, q_out, mq_ref, qb_ref, q_terms, early, rows_in - early)
        send_block(q_out, early, rows_in - early)
    own_update(k_step, k_new, k_out, mk_ref, kb_ref, k_terms, 0, rows_in)
    send_block(k_out, 0, rows_in)

    @pl.when(row != height)
    def _():
        spread_copy(1).wait_recv()

    swap_b = sender.start(blocks_b, pair_b, pair)
    for name in ("bf", "bs", "mb"):
        loads[name].wait()
    swap_b.wait_recv()

    def branch_low(held):
        return [unpack_columns(held[n, :wide, :], held[n, wide:, :]) for n in range(nf)]

    mine, theirs = branch_low(blocks_b), branch_low(pair_b)
    for place in range(2):
        here = core == place
        for n in range(nf):
            low = jnp.where(here, mine[n], theirs[n])
            rows = slice(place * features + n * wide, place * features + (n + 1) * wide)
            bf_out[rows, :], bs_out[rows, :], b_dir = moments(bf_ref[rows, :], bs_ref[rows, :], low, clip)
            step = sum(
                jnp.dot(term, bbt_ref[...], preferred_element_type=jnp.float32)
                for term in split_two(b_dir)
            )
            b_step[rows, :] = step
            updated = mb_ref[rows, :] - LEARN * step
            b_new[rows, :] = updated
            b_out[row, rows, :] = updated.astype(b_out.dtype)
    send_block(b_out, 0, rows_in)

    own_update(q_step, q_new, q_out, mq_ref, qb_ref, q_terms, 0, early)
    for copy in sent[2:] + passed:
        copy.wait_recv()
    for o in range(1, nf):
        source = lax.rem(row + o, nf)
        step = exact_dot(basis_rows(qb_ref, source, 0, early), q_terms)
        master = decoded(far[source], MASTER_POWER) * (1.0 / MASTER_GAIN)
        q_out[source, :early, :] = (master - LEARN * step).astype(q_out.dtype)

    last = []
    for n, h, out, target, copy in late:
        copy.wait_recv()
        if n == h:
            held = out.at[(side, front)[n], target]
            last.append(sender.start(held, held, names[1 - n]))
    for copy in last:
        copy.wait_recv()
    sender.drain()

    @pl.when(row != height)
    def _():
        to_block(own_b, blocks_b.at[row]).wait_send()

    @pl.when(row == height)
    def _():
        for o in range(1, nz):
            spread_copy(o).wait_send()


def fused(nf, nt, early, *args):
    x, qu, ku, h, bu, mq, mk, mb, qb, kb, bb, qf, qs, kf, ks, bf, bs = args
    tokens, features = x.shape
    rank = qb.shape[1]
    half, nz = tokens // 2, nt // 2
    piece, thin, wide = half // nz, rank // nf, features // nf
    cols = qu.shape[1] + ku.shape[1]
    coded_rows = 3 * rank + 48
    count = 80
    f32, b16 = jnp.float32, jnp.bfloat16
    vmem = pltpu.VMEM
    outs = [vmem(m.shape, f32) for m in (mq, mk, mb)] * 2
    outs += [vmem((nf, *m.shape), b16) for m in (mq, mk, mb)]
    outs += [vmem(m.shape, f32) for m in (qf, qs, kf, ks, bf, bs)]
    held = (x, qu, ku, h, bu, mq, mk, mb, qb, kb, qf, qs, kf, ks, bf, bs)
    results = pl.pallas_call(
        functools.partial(fused_kernel, nf, nt, early),
        out_shape=tuple(outs),
        in_specs=[pl.BlockSpec(memory_space=pl.ANY)] * len(args),
        out_specs=(pl.BlockSpec(memory_space=pltpu.VMEM),) * len(outs),
        scratch_shapes=[
            *[vmem(a.shape, a.dtype) for a in held],
            vmem((3, features, rank), b16),
            vmem((3 * rank, features), b16),
            vmem((rank, features), b16),
            vmem((3 * rank, half), f32),
            vmem((3 * rank, half), f32),
            vmem((nz, 3 * rank, piece), f32),
            vmem((nz, coded_rows, piece), b16),
            vmem((nz - 1, coded_rows, piece), b16),
            vmem((nz, coded_rows, piece), b16),
            vmem((nz, coded_rows, piece), b16),
            vmem((3, 2 * rank, half), b16),
            vmem((nf, thin, cols), f32),
            vmem((nf, rank, wide), f32),
            vmem((nf - 1, thin, cols), f32),
            vmem((nf - 1, rank, wide), f32),
            vmem((nf, thin, cols), f32),
            vmem((wide + 16, rank), b16),
            vmem((nf, wide + 16, rank), b16),
            vmem((nf, wide + 16, rank), b16),
            vmem((nf, 8, 128), f32),
            vmem((nt, 8, 128), f32),
            vmem((early, mq.shape[1]), b16),
            vmem((nf, early, mq.shape[1]), b16),
            pltpu.SemaphoreType.DMA((count,)),
            pltpu.SemaphoreType.DMA((count,)),
            pltpu.SemaphoreType.DMA((32,)),
            pltpu.SemaphoreType.DMA((nf + 1,)),
        ],
        compiler_params=pltpu.CompilerParams(
            collective_id=0, has_side_effects=True, vmem_limit_bytes=VMEM_LIMIT
        ),
    )(*args)
    results = list(results)
    results[6:9] = [r.reshape(-1, r.shape[-1]) for r in results[6:9]]
    return tuple(results)


def per_device(
    normed_inputs,
    query_upstream,
    key_upstream,
    head_outputs,
    branch_upstream,
    query_master,
    key_master,
    branch_master,
    query_basis,
    key_basis,
    branch_basis,
    query_first,
    query_second,
    key_first,
    key_second,
    branch_first,
    branch_second,
):
    exact = lax.Precision.HIGHEST
    row_index = lax.axis_index("fs")
    col_index = lax.axis_index("tp")
    n_rows = lax.axis_size("fs")
    n_cols = lax.axis_size("tp")
    features = normed_inputs.shape[1]
    query_local = query_upstream.shape[1]
    key_local = key_upstream.shape[1]
    rows_in = query_master.shape[0]
    rank = query_basis.shape[1]
    even = n_cols == 2 * n_rows and features * 2 == rows_in and key_local % 128 == 0
    if n_rows == 4 and even and features % 512 == 0 and normed_inputs.shape[0] % 1024 == 0:
        return fused(
            n_rows, n_cols, rows_in // 64 * EARLY_OF_64, normed_inputs, query_upstream, key_upstream,
            head_outputs, branch_upstream, query_master, key_master, branch_master,
            query_basis, key_basis, branch_basis, query_first, query_second,
            key_first, key_second, branch_first, branch_second,
        )

    def own_block(basis):
        return lax.dynamic_slice_in_dim(basis, col_index * features, features, 0)

    block_branch = own_block(branch_basis)
    own_branch = block_branch.astype(jnp.float32)
    lanes = -key_local % 128
    early = rows_in // 32 * 20
    low, branch_low, squares, far = reduced(
        n_rows,
        n_cols,
        early,
        normed_inputs,
        query_upstream,
        jnp.pad(key_upstream, ((0, 0), (0, lanes))),
        head_outputs,
        branch_upstream,
        query_master,
        own_block(query_basis),
        own_block(key_basis),
        block_branch,
    )
    query_low = low[:, :query_local]
    key_low = low[:, query_local : query_local + key_local]
    branch_low = branch_low.reshape(branch_first.shape)
    total = squares[0, 0]
    entries = rank * n_cols * (2 * query_local + key_local)
    rms_value = jnp.sqrt(total / float(entries))
    clip = 1.0 / jnp.maximum(1.0, rms_value / CLIP_RMS)
    q_first, q_second, q_dir = moments(query_first, query_second, query_low, clip)
    k_first, k_second, k_dir = moments(key_first, key_second, key_low, clip)
    b_first, b_second, b_dir = moments(branch_first, branch_second, branch_low, clip)
    step_rows_query = lax.dynamic_slice_in_dim(query_basis, row_index * rows_in, rows_in, 0).astype(
        jnp.float32
    )
    step_rows_key = lax.dynamic_slice_in_dim(key_basis, row_index * rows_in, rows_in, 0).astype(
        jnp.float32
    )
    query_step = jnp.dot(step_rows_query, q_dir, precision=exact)
    key_step = jnp.dot(step_rows_key, k_dir, precision=exact)
    branch_step = jnp.dot(b_dir, own_branch.T, precision=exact)
    query_updated = query_master - LEARN * query_step
    key_updated = key_master - LEARN * key_step
    branch_updated = branch_master - LEARN * branch_step
    query_copy, branch_copy, key_copy = gathered_rows(
        n_rows,
        n_cols,
        query_updated[early:].astype(jnp.bfloat16),
        branch_updated.astype(jnp.bfloat16),
        jnp.pad(key_updated, ((0, 0), (0, lanes))).astype(jnp.bfloat16),
        far,
        query_master,
        query_basis,
        q_dir,
    )
    key_copy = key_copy[:, :key_local]
    return (
        query_step,
        key_step,
        branch_step,
        query_updated,
        key_updated,
        branch_updated,
        query_copy,
        key_copy,
        branch_copy,
        q_first,
        q_second,
        k_first,
        k_second,
        b_first,
        b_second,
    )


def solution(mesh):
    return jax.shard_map(
        per_device,
        mesh=mesh,
        in_specs=(
            P("fs", "tp"),
            P("fs", "tp"),
            P("fs", "tp"),
            P("fs", "tp"),
            P("fs", "tp"),
            P("fs", "tp"),
            P("fs", "tp"),
            P("fs", "tp"),
            P(),
            P(),
            P(),
            P(None, "tp"),
            P(None, "tp"),
            P(None, "tp"),
            P(None, "tp"),
            P("fs", None),
            P("fs", None),
        ),
        out_specs=(
            P("fs", "tp"),
            P("fs", "tp"),
            P("fs", "tp"),
            P("fs", "tp"),
            P("fs", "tp"),
            P("fs", "tp"),
            P(None, "tp"),
            P(None, "tp"),
            P(None, "tp"),
            P(None, "tp"),
            P(None, "tp"),
            P(None, "tp"),
            P(None, "tp"),
            P("fs", None),
            P("fs", None),
        ),
        check_vma=False,
    )
```

```python
import functools

import jax
import jax.numpy as jnp
from jax import lax
from jax.experimental import pallas as pl
from jax.experimental.pallas import tpu as pltpu
from jax.sharding import PartitionSpec as P

LEARN = 0.02
BETA_ONE = 0.9
BETA_TWO = 0.95
ADAM_EPS = 1e-08
CLIP_RMS = 0.5


def moments(first, second, low, clip):
    scaled = clip * low
    first_new = BETA_ONE * first + (1.0 - BETA_ONE) * scaled
    second_new = BETA_TWO * second + (1.0 - BETA_TWO) * scaled * scaled
    return (first_new, second_new, first_new / (jnp.sqrt(second_new) + ADAM_EPS))


def over_tokens(left, right, precision=None):
    return lax.dot_general(
        left,
        right,
        (((0,), (0,)), ((), ())),
        precision=precision,
        preferred_element_type=jnp.float32,
    )


def split_three(values):
    high = values.astype(jnp.bfloat16)
    rest = values - high.astype(jnp.float32)
    middle = rest.astype(jnp.bfloat16)
    low = (rest - middle.astype(jnp.float32)).astype(jnp.bfloat16)
    return high, middle, low


class Sender:
    def __init__(self, send_sem, recv_sem):
        self.send_sem, self.recv_sem, self.used, self.started = send_sem, recv_sem, 0, []

    def reserve(self, count):
        self.used += count
        return self.used - count

    def start(self, source, target, device):
        copy = pltpu.make_async_remote_copy(
            src_ref=source,
            dst_ref=target,
            send_sem=self.send_sem.at[self.used],
            recv_sem=self.recv_sem.at[self.used],
            device_id=device,
            device_id_type=pl.DeviceIdType.MESH,
        )
        self.used += 1
        copy.start()
        self.started.append(copy)
        return copy

    def drain(self):
        for copy in self.started:
            copy.wait_send()


def greet(nf, nt, row, col, both):
    barrier = pltpu.get_barrier_semaphore()
    peers = [{"fs": lax.rem(row + o, nf), "tp": col} for o in range(1, nf)]
    if both:
        peers += [{"fs": row, "tp": lax.rem(col + o, nt)} for o in range(1, nt)]
    for peer in peers:
        pl.semaphore_signal(
            barrier, inc=1, device_id=peer, device_id_type=pl.DeviceIdType.MESH
        )
    pl.semaphore_wait(barrier, len(peers))


def square(row, col):
    side = row + 1 - 2 * lax.rem(row, 2)
    front = lax.rem(row + 2, 4)
    return side, front, ({"fs": side, "tp": col}, {"fs": front, "tp": col})


def reduce_kernel(
    nf, nt,
    x_hbm, qu_hbm, ku_hbm, h_hbm, bu_hbm, master_ref, qb_ref, kb_ref, bb_ref,
    qk_out, b_out, total_out, far_out,
    x_ref, qu_ref, ku_ref, h_ref, bu_ref,
    part, from_pair, halves, arrived, whole, other,
    part_qk, part_b, got_qk, got_b, all_qk, all_b, spread_b, sums,
    send_sem, recv_sem, load_sem,
):
    row, col = lax.axis_index("fs"), lax.axis_index("tp")
    core, height = lax.rem(col, 2), lax.div(col, 2)
    nz = nt // 2
    rank = qb_ref.shape[1]
    half = x_ref.shape[0] // 2
    piece = half // nz
    query_cols = qu_ref.shape[1]
    loads = []

    def load(source, target):
        copy = pltpu.make_async_copy(source, target, load_sem.at[len(loads)])
        copy.start()
        loads.append(copy)

    for which in (1 - core, core):
        rows = pl.ds(pl.multiple_of(which * half, half), half)
        load(x_hbm.at[rows], x_ref.at[rows])
        load(bu_hbm.at[rows], bu_ref.at[rows])
    load(qu_hbm, qu_ref)
    load(ku_hbm, ku_ref)
    load(h_hbm, h_ref)
    greet(nf, nt, row, col, True)
    sender = Sender(send_sem, recv_sem)
    pair = {"fs": row, "tp": height * 2 + (1 - core)}

    def above(o):
        return {"fs": row, "tp": lax.rem(height + o, nz) * 2 + core}

    def beside(o):
        return {"fs": lax.rem(row + o, nf), "tp": col}

    def project(which):
        rows = pl.ds(pl.multiple_of(which * half, half), half)
        x = x_ref[rows, :]
        return (
            jnp.dot(x, qb_ref[...], preferred_element_type=jnp.float32),
            jnp.dot(x, kb_ref[...], preferred_element_type=jnp.float32),
            jnp.dot(bu_ref[rows, :], bb_ref[...], preferred_element_type=jnp.float32),
        )

    early = far_out.shape[1]
    sent = []
    if nf == 4:
        side, front, names = square(row, col)
        for turn in range(2):
            for n in range(2):
                rows = pl.ds((turn ^ n) * (early // 2), early // 2)
                sent.append(
                    sender.start(master_ref.at[rows], far_out.at[row, rows], names[n])
                )
    else:
        rows = pl.ds(0, early)
        for o in range(1, nf):
            sent.append(sender.start(master_ref.at[rows], far_out.at[row], beside(o)))
    loads[0].wait()
    loads[1].wait()
    for n, value in enumerate(project(1 - core)):
        part[:, n * rank : (n + 1) * rank] = value
    swap = sender.start(part, from_pair, pair)
    loads[2].wait()
    loads[3].wait()
    own = project(core)
    swap.wait_recv()
    for n, value in enumerate(own):
        span = slice(n * rank, (n + 1) * rank)
        halves[:, :, span] = (value + from_pair[:, span]).reshape(nz, piece, rank)
    copies = [
        sender.start(halves.at[lax.rem(height + o, nz)], arrived.at[o - 1], above(o))
        for o in range(1, nz)
    ]
    total = halves[height]
    for o, copy in enumerate(copies):
        copy.wait_recv()
        total = total + arrived[o]
    whole[height] = total
    copies = [sender.start(whole.at[height], whole.at[height], above(o)) for o in range(1, nz)]
    across = [sender.start(whole.at[height], other.at[height], pair)]
    passed = []
    if nf == 4:
        for n, source in ((0, side), (1, front)):
            sent[n].wait_recv()
            held = far_out.at[source, pl.ds(n * (early // 2), early // 2)]
            passed.append(sender.start(held, held, names[1 - n]))
    for o, copy in enumerate(copies, 1):
        copy.wait_recv()
        source = lax.rem(height + nz - o, nz)
        across.append(sender.start(whole.at[source], other.at[source], pair))

    over_rows = (((0,), (0,)), ((), ()))

    def low_parts(values, which):
        rows = pl.ds(pl.multiple_of(which * half, half), half)
        sides = (qu_ref[rows, :], ku_ref[rows, :], h_ref[rows, :])
        parts = []
        for n, side in enumerate(sides):
            terms = split_three(values[:, n * rank : (n + 1) * rank])
            parts.append(
                sum(
                    lax.dot_general(term, side, over_rows, preferred_element_type=jnp.float32)
                    for term in terms
                )
            )
        return parts

    for copy in loads[4:]:
        copy.wait()
    first = low_parts(whole[...].reshape(half, 3 * rank), core)
    for copy in across:
        copy.wait_recv()
    second = low_parts(other[...].reshape(half, 3 * rank), 1 - core)
    query_part, key_part, branch_part = [a + b for a, b in zip(first, second)]
    part_qk[:, :, :query_cols] = query_part.reshape(nf, rank // nf, query_cols)
    part_qk[:, :, query_cols:] = key_part.reshape(nf, rank // nf, key_part.shape[1])
    part_b[...] = branch_part.T.reshape(part_b.shape)

    copies = []
    for o in range(1, nf):
        to = lax.rem(row + o, nf)
        copies.append(sender.start(part_qk.at[to], got_qk.at[o - 1], beside(o)))
        copies.append(sender.start(part_b.at[to], got_b.at[o - 1], beside(o)))
    for copy in copies:
        copy.wait_recv()
    sum_qk, sum_b = part_qk[row], part_b[row]
    for o in range(nf - 1):
        sum_qk = sum_qk + got_qk[o]
        sum_b = sum_b + got_b[o]
    rows_b = sum_b.shape[0]
    squares = jnp.sum(sum_qk * sum_qk) + jnp.sum(sum_b * sum_b)
    all_qk[row] = sum_qk
    all_b[col, :rows_b, :] = sum_b
    all_b[col, rows_b:, :] = jnp.full((8, rank), squares, jnp.float32)

    copies_b = [
        sender.start(all_b.at[col], all_b.at[col], {"fs": row, "tp": lax.rem(col + o, nt)})
        for o in range(1, nt)
    ]
    copies_qk = [sender.start(all_qk.at[row], all_qk.at[row], beside(o)) for o in range(1, nf)]
    for copy in copies_b:
        copy.wait_recv()
    sums[row] = jnp.sum(all_b[:, rows_b:, :], axis=0)
    each = nt // nf
    copies = []
    for o in range(1, nf):
        blocks = pl.ds(lax.rem(row + o, nf) * each, each)
        copies.append(sender.start(sums.at[row], sums.at[row], beside(o)))
        copies.append(sender.start(all_b.at[blocks], spread_b.at[row], beside(o)))
    b_out[:, row] = all_b[pl.ds(row * each, each)][:, :rows_b, :]
    for copy in copies_qk:
        copy.wait_recv()
    qk_out[...] = all_qk[...].reshape(qk_out.shape)
    for copy in copies:
        copy.wait_recv()
    for o in range(1, nf):
        source = lax.rem(row + o, nf)
        b_out[:, source] = spread_b[source][:, :rows_b, :]
    total_out[...] = jnp.sum(sums[...], axis=0)
    for copy in (sent[2:] + passed) if nf == 4 else sent:
        copy.wait_recv()
    sender.drain()


def reduced(nf, nt, early, x, qu, ku, h, bu, master, qb, kb, bb):
    tokens, features = x.shape
    rank = qb.shape[1]
    cols = qu.shape[1] + ku.shape[1]
    half, nz, each = tokens // 2, nt // 2, nt // nf
    piece, thin, rows_b = half // nz, rank // nf, features // nf
    copies = 1 + 2 * (nz - 1) + nz + 2 * (nf - 1) + (nt - 1) + 3 * (nf - 1)
    copies += 6 if nf == 4 else nf - 1
    any_place = pl.BlockSpec(memory_space=pl.ANY)
    vmem = pl.BlockSpec(memory_space=pltpu.VMEM)
    f32 = jnp.float32
    return pl.pallas_call(
        functools.partial(reduce_kernel, nf, nt),
        out_shape=(
            jax.ShapeDtypeStruct((rank, cols), f32),
            jax.ShapeDtypeStruct((each, nf, rows_b, rank), f32),
            jax.ShapeDtypeStruct((8, rank), f32),
            jax.ShapeDtypeStruct((nf, early, master.shape[1]), f32),
        ),
        in_specs=[any_place] * 6 + [vmem] * 3,
        out_specs=(vmem, vmem, vmem, any_place),
        scratch_shapes=[
            *[pltpu.VMEM(each_in.shape, each_in.dtype) for each_in in (x, qu, ku, h, bu)],
            pltpu.VMEM((half, 3 * rank), f32),
            pltpu.VMEM((half, 3 * rank), f32),
            pltpu.VMEM((nz, piece, 3 * rank), f32),
            pltpu.VMEM((nz - 1, piece, 3 * rank), f32),
            pltpu.VMEM((nz, piece, 3 * rank), f32),
            pltpu.VMEM((nz, piece, 3 * rank), f32),
            pltpu.VMEM((nf, thin, cols), f32),
            pltpu.VMEM((nf, rows_b, rank), f32),
            pltpu.VMEM((nf - 1, thin, cols), f32),
            pltpu.VMEM((nf - 1, rows_b, rank), f32),
            pltpu.VMEM((nf, thin, cols), f32),
            pltpu.VMEM((nt, rows_b + 8, rank), f32),
            pltpu.VMEM((nf, each, rows_b + 8, rank), f32),
            pltpu.VMEM((nf, 8, rank), f32),
            pltpu.SemaphoreType.DMA((copies,)),
            pltpu.SemaphoreType.DMA((copies,)),
            pltpu.SemaphoreType.DMA((7,)),
        ],
        compiler_params=pltpu.CompilerParams(
            collective_id=0, has_side_effects=True, vmem_limit_bytes=58 * 2**20
        ),
    )(x, qu, ku, h, bu, master, qb, kb, bb)


def gather_kernel(
    nf, nt,
    q_ref, b_ref, k_ref, far_ref, master_ref, basis_ref, dir_ref,
    q_out, b_out, k_out,
    held_far, held_copy, send_sem, recv_sem, own_sem, load_sem, store_sem,
):
    row, col = lax.axis_index("fs"), lax.axis_index("tp")
    early = far_ref.shape[1]
    pairs = ((q_ref, q_out, early), (b_ref, b_out, 0), (k_ref, k_out, 0))

    def load(o):
        source = master_ref.at[pl.ds(0, early)] if o == 0 else far_ref.at[lax.rem(row + o, nf)]
        copy = pltpu.make_async_copy(source, held_far.at[o % 2], load_sem.at[o])
        copy.start()
        return copy

    coming = load(0)
    greet(nf, nt, row, col, False)
    sender = Sender(send_sem, recv_sem)
    sent = []
    if nf == 4:
        side, front, names = square(row, col)
        for ref, out, base in pairs:
            half = ref.shape[0] // 2
            for h in range(2):
                rows = pl.ds(h * half, half)
                target = pl.ds(base + h * half, half)
                for n in ((0, 1), (1, 0))[h]:
                    copy = sender.start(ref.at[rows], out.at[row, target], names[n])
                    sent.append((n, h, out, target, copy))
    else:
        for ref, out, base in pairs:
            for o in range(1, nf):
                target = out.at[row, pl.ds(base, ref.shape[0])]
                there = {"fs": lax.rem(row + o, nf), "tp": col}
                sent.append(sender.start(ref, target, there))
    local = []
    for n, (ref, out, base) in enumerate(pairs):
        target = out.at[row, pl.ds(base, ref.shape[0])]
        local.append(pltpu.make_async_copy(ref, target, own_sem.at[n]))
        local[-1].start()

    terms = split_three(dir_ref[...])
    rows_all = q_out.shape[1]
    stores = []
    for o in range(nf):
        source = lax.rem(row + o, nf)
        coming.wait()
        if o + 1 < nf:
            coming = load(o + 1)
        if o >= 2:
            stores[o - 2].wait()
        basis = basis_ref[pl.ds(pl.multiple_of(source * rows_all, rows_all), early), :]
        step = sum(jnp.dot(basis, term, preferred_element_type=jnp.float32) for term in terms)
        held_copy[o % 2] = (held_far[o % 2] - LEARN * step).astype(held_copy.dtype)
        stores.append(
            pltpu.make_async_copy(
                held_copy.at[o % 2], q_out.at[source, pl.ds(0, early)], store_sem.at[o]
            )
        )
        stores[-1].start()

    if nf == 4:
        last = []
        for n, h, out, target, copy in sent:
            copy.wait_recv()
            if n == h:
                held = out.at[(side, front)[n], target]
                last.append(sender.start(held, held, names[1 - n]))
        sent = last
    for copy in sent:
        copy.wait_recv()
    for copy in local + stores[-2:]:
        copy.wait()
    sender.drain()


def gathered_rows(nf, nt, q_tail, b_block, k_block, far, master, basis, direction):
    count = 18 if nf == 4 else 3 * (nf - 1)
    early = far.shape[1]
    blocks = (master, b_block, k_block)
    wide = [jax.ShapeDtypeStruct((nf, *block.shape), q_tail.dtype) for block in blocks]
    vmem = pl.BlockSpec(memory_space=pltpu.VMEM)
    any_place = pl.BlockSpec(memory_space=pl.ANY)
    outs = pl.pallas_call(
        functools.partial(gather_kernel, nf, nt),
        out_shape=tuple(wide),
        in_specs=[vmem] * 3 + [any_place] * 2 + [vmem] * 2,
        out_specs=(any_place,) * 3,
        scratch_shapes=[
            pltpu.VMEM((2, early, far.shape[2]), far.dtype),
            pltpu.VMEM((2, early, far.shape[2]), q_tail.dtype),
            pltpu.SemaphoreType.DMA((count,)),
            pltpu.SemaphoreType.DMA((count,)),
            pltpu.SemaphoreType.DMA((3,)),
            pltpu.SemaphoreType.DMA((nf,)),
            pltpu.SemaphoreType.DMA((nf,)),
        ],
        compiler_params=pltpu.CompilerParams(
            collective_id=1, has_side_effects=True, vmem_limit_bytes=48 * 2**20
        ),
    )(q_tail, b_block, k_block, far, master, basis, direction)
    return [out.reshape(-1, out.shape[-1]) for out in outs]


EARLY_OF_64 = 64
PASSED_OF_16 = (8, 12)
VMEM_LIMIT = 40 * 2**20
MASTER_MOST = 0.09375
MASTER_POWER = 14
MASTER_GAIN = 515.0 / MASTER_MOST
SUM_POWER = 16
SUM_GAIN = 238.0


def raised(magnitude, power):
    result, square = None, magnitude
    while power:
        if power % 2:
            result = square if result is None else result * square
        power //= 2
        if power:
            square = square * square
    return result


def coded(values, power):
    high = raised(jnp.abs(values), power)
    return jnp.where(values < 0, -high, high).astype(jnp.bfloat16)


def decoded(codes, power):
    codes = codes.astype(jnp.float32)
    root = jnp.exp(jnp.log(jnp.abs(codes)) * (1.0 / power))
    root = jnp.where(codes == 0, 0.0, root)
    return jnp.where(codes < 0, -root, root)


def pack(values, axis):
    most = jnp.max(jnp.abs(values), axis=axis, keepdims=True)
    scale = jnp.maximum(most, 1e-30).astype(jnp.bfloat16).astype(jnp.float32)
    return coded(values * (SUM_GAIN / scale), SUM_POWER), scale


def unpack(codes, scale):
    return decoded(codes, SUM_POWER) * (scale.astype(jnp.float32) * (1.0 / SUM_GAIN))


def pack_columns(values):
    codes, scale = pack(values, 0)
    return codes, jnp.broadcast_to(scale, (16, values.shape[1])).astype(jnp.bfloat16)


def unpack_columns(codes, scale):
    return unpack(codes, scale[0:1])


def stacked(scales, width):
    place = lax.broadcasted_iota(jnp.int32, (16, width), 0)
    rows = jnp.broadcast_to(scales[-1], (16, width))
    for n, scale in enumerate(scales[:-1]):
        rows = jnp.where(place == n, scale, rows)
    return rows.astype(jnp.bfloat16)


def split_two(values):
    high = values.astype(jnp.bfloat16)
    return high, (values - high.astype(jnp.float32)).astype(jnp.bfloat16)


def exact_dot(left, terms):
    return sum(jnp.dot(left, term, preferred_element_type=jnp.float32) for term in terms)


def fused_kernel(
    nf, nt, early,
    x_hbm, qu_hbm, ku_hbm, h_hbm, bu_hbm, mq_hbm, mk_hbm, mb_hbm, qb_hbm, kb_hbm, bb_hbm,
    qf_hbm, qs_hbm, kf_hbm, ks_hbm, bf_hbm, bs_hbm,
    q_step, k_step, b_step, q_new, k_new, b_new, q_out, k_out, b_out,
    qf_out, qs_out, kf_out, ks_out, bf_out, bs_out,
    x_ref, qu_ref, ku_ref, h_ref, bu_ref, mq_ref, mk_ref, mb_ref, qb_ref, kb_ref,
    qf_ref, qs_ref, kf_ref, ks_ref, bf_ref, bs_ref, own_ref, turned, bbt_ref,
    part, from_pair, halves, sent_z, arrived, whole, other, split_ref,
    part_qk, part_b, sent_qk, sent_b, got_qk, got_b, all_qk, own_b, blocks_b, pair_b, sums_f, sums_t,
    enc, far,
    send_sem, recv_sem, load_sem, b_recv,
):
    row, col = lax.axis_index("fs"), lax.axis_index("tp")
    core, height = lax.rem(col, 2), lax.div(col, 2)
    nz = nt // 2
    rank = qb_ref.shape[1]
    tokens, features = x_ref.shape
    half = tokens // 2
    piece = half // nz
    query_cols, key_cols = qu_ref.shape[1], ku_ref.shape[1]
    rows_in = mq_ref.shape[0]
    loads = {}

    def load(name, source, target):
        copy = pltpu.make_async_copy(source, target, load_sem.at[len(loads)])
        copy.start()
        loads[name] = copy

    needed = set()

    def need(*keys):
        for key in keys:
            if key not in needed:
                needed.add(key)
                loads[key].wait()

    def token_rows(which):
        return pl.ds(pl.multiple_of(which * half, half), half)

    first, second = pl.ds(0, early // 2), pl.ds(early // 2, early // 2)
    load("mq0", mq_hbm.at[first], mq_ref.at[first])
    load("mq1", mq_hbm.at[second], mq_ref.at[second])
    own_rows = pl.ds(pl.multiple_of(col * features, features), features)
    for n, basis in enumerate((qb_hbm, kb_hbm, bb_hbm)):
        load(("own", n), basis.at[own_rows], own_ref.at[n])
    for n, which in enumerate((1 - core, core)):
        load(("x", n), x_hbm.at[token_rows(which)], x_ref.at[token_rows(which)])
        load(("bu", n), bu_hbm.at[token_rows(which)], bu_ref.at[token_rows(which)])
    load("qu", qu_hbm, qu_ref)
    load("ku", ku_hbm, ku_ref)
    load("h", h_hbm, h_ref)
    if early < rows_in:
        rest = pl.ds(early, rows_in - early)
        load("mq2", mq_hbm.at[rest], mq_ref.at[rest])
    for name, source, target in (
        ("qf", qf_hbm, qf_ref), ("qs", qs_hbm, qs_ref), ("kf", kf_hbm, kf_ref), ("ks", ks_hbm, ks_ref),
        ("qb", qb_hbm, qb_ref), ("kb", kb_hbm, kb_ref), ("mk", mk_hbm, mk_ref),
        ("bf", bf_hbm, bf_ref), ("bs", bs_hbm, bs_ref), ("mb", mb_hbm, mb_ref),
    ):
        load(name, source, target)

    greet(nf, nt, row, col, True)
    sender = Sender(send_sem, recv_sem)
    pair = {"fs": row, "tp": height * 2 + (1 - core)}
    side, front, names = square(row, col)

    def above(o):
        return {"fs": row, "tp": lax.rem(height + o, nz) * 2 + core}

    def beside(o):
        return {"fs": lax.rem(row + o, nf), "tp": col}

    parts = (first, second)
    sent = []
    for turn in range(2):
        if turn == 0:
            for n in range(2):
                need(f"mq{n}")
                enc[parts[n], :] = coded(mq_ref[parts[n], :] * MASTER_GAIN, MASTER_POWER)
        for n in range(2):
            rows = parts[turn ^ n]
            sent.append(sender.start(enc.at[rows], far.at[row, rows], names[n]))

    for n in range(3):
        need(("own", n))
        turned[n * rank : (n + 1) * rank, :] = own_ref[n].T

    def project(n, which):
        need(("x", n), ("bu", n))
        over = (((1,), (1,)), ((), ()))
        a = lax.dot_general(turned[: 2 * rank, :], x_ref[token_rows(which), :], over, preferred_element_type=jnp.float32)
        b = lax.dot_general(turned[2 * rank :, :], bu_ref[token_rows(which), :], over, preferred_element_type=jnp.float32)
        return a, b

    a, b = project(0, 1 - core)
    part[: 2 * rank, :] = a
    part[2 * rank :, :] = b
    swap = sender.start(part, from_pair, pair)
    a, b = project(1, core)
    swap.wait_recv()
    for n in range(nz):
        span = slice(n * piece, (n + 1) * piece)
        halves[n, : 2 * rank, :] = a[:, span] + from_pair[: 2 * rank, span]
        halves[n, 2 * rank :, :] = b[:, span] + from_pair[2 * rank :, span]

    def put(target, n, values):
        scales = []
        for k in range(3):
            codes, scale = pack(values[k], 0)
            target[n, k * rank : (k + 1) * rank, :] = codes
            scales.append(scale)
        target[n, 3 * rank :, :] = stacked(scales, piece)

    def take(source, n, k):
        scale = source[n, 3 * rank :, :].astype(jnp.float32)[k : k + 1]
        return unpack(source[n, k * rank : (k + 1) * rank, :], scale)

    def thirds(values):
        return [values[k * rank : (k + 1) * rank] for k in range(3)]

    copies = []
    for o in range(1, nz):
        to = lax.rem(height + o, nz)
        put(sent_z, to, thirds(halves[to]))
        copies.append(sender.start(sent_z.at[to], arrived.at[o - 1], above(o)))
    for copy in copies:
        copy.wait_recv()
    totals = thirds(halves[height])
    for k in range(3):
        for o in range(nz - 1):
            totals[k] = totals[k] + take(arrived, o, k)
    put(whole, height, totals)
    copies = [sender.start(whole.at[height], whole.at[height], above(o)) for o in range(1, nz)]
    across = [sender.start(whole.at[height], other.at[height], pair)]

    passed = []

    def pass_on(begin, end):
        unit = early // 32
        for n, source in ((0, side), (1, front)):
            held = far.at[source, pl.ds(n * (early // 2) + begin * unit, (end - begin) * unit)]
            passed.append(sender.start(held, held, names[1 - n]))

    for n in range(2):
        sent[n].wait_recv()
    pass_on(0, PASSED_OF_16[0])

    bbt_ref[...] = turned[2 * rank :, :]
    for o, copy in enumerate(copies, 1):
        copy.wait_recv()
        source = lax.rem(height + nz - o, nz)
        across.append(sender.start(whole.at[source], other.at[source], pair))

    def low_parts(held, which):
        for n in range(nz):
            for k in range(3):
                high, low = split_two(take(held, n, k))
                split_ref[k, :rank, n * piece : (n + 1) * piece] = high
                split_ref[k, rank:, n * piece : (n + 1) * piece] = low
        lows = []
        for k, ref in enumerate((qu_ref, ku_ref, h_ref)):
            both = jnp.dot(split_ref[k], ref[token_rows(which), :], preferred_element_type=jnp.float32)
            lows.append(both[:rank] + both[rank:])
        return lows

    need("qu", "ku", "h")
    one = low_parts(whole, core)
    for copy in across:
        copy.wait_recv()
    two = low_parts(other, 1 - core)
    thin, wide = rank // nf, features // nf
    query_part, key_part, branch_part = [a + b for a, b in zip(one, two)]
    cols = query_cols + key_cols

    def put_qk(query, key):
        query_codes, query_scale = pack(query, 1)
        key_codes, key_scale = pack(key, 1)
        place = lax.broadcasted_iota(jnp.int32, (query.shape[0], 128), 1)
        scale = jnp.where(place < 64, query_scale, key_scale).astype(jnp.bfloat16)
        return ((slice(0, query_cols), query_codes), (slice(query_cols, cols), key_codes), (slice(cols, cols + 128), scale))

    def take_qk(held):
        scale = held[:, cols:].astype(jnp.float32)
        return unpack(held[:, :query_cols], scale[:, 0:1]), unpack(held[:, query_cols:cols], scale[:, 64:65])

    for span, values in put_qk(query_part, key_part):
        sent_qk[:, :, span] = values.reshape(nf, thin, values.shape[1])
    part_qk[:, :, :query_cols] = query_part.reshape(nf, thin, query_cols)
    part_qk[:, :, query_cols:] = key_part.reshape(nf, thin, key_cols)
    codes, scale = pack_columns(branch_part)
    for n in range(nf):
        part_b[n] = branch_part[:, n * wide : (n + 1) * wide]
        sent_b[n, :rank, :] = codes[:, n * wide : (n + 1) * wide]
        sent_b[n, rank:, :] = scale[:, n * wide : (n + 1) * wide]

    copies = []
    for o in range(1, nf):
        to = lax.rem(row + o, nf)
        copies.append(sender.start(sent_qk.at[to], got_qk.at[o - 1], beside(o)))
        copies.append(sender.start(sent_b.at[to], got_b.at[o - 1], beside(o)))
    pass_on(*PASSED_OF_16)
    for copy in copies:
        copy.wait_recv()
    sum_q, sum_k, sum_b = part_qk[row, :, :query_cols], part_qk[row, :, query_cols:], part_b[row]
    for o in range(nf - 1):
        got_query, got_key = take_qk(got_qk[o])
        sum_q, sum_k = sum_q + got_query, sum_k + got_key
        sum_b = sum_b + unpack_columns(got_b[o, :rank, :], got_b[o, rank:, :])
    squares = jnp.sum(sum_q * sum_q) + jnp.sum(sum_k * sum_k) + jnp.sum(sum_b * sum_b)
    sums_f[row] = jnp.full((8, 128), squares, jnp.float32)
    copies_s = [sender.start(sums_f.at[row], sums_f.at[row], beside(o)) for o in range(1, nf)]
    for span, values in put_qk(sum_q, sum_k):
        all_qk[row, :, span] = values
    copies_qk = [sender.start(all_qk.at[row], all_qk.at[row], beside(o)) for o in range(1, nf)]
    sum_b = sum_b.T
    codes, scale = pack_columns(sum_b)
    own_b[:wide, :] = codes
    own_b[wide:, :] = scale

    spread = sender.reserve(nz - 1)
    to_owner = sender.reserve(1)
    owner = {"fs": height, "tp": col}

    def to_block(source, target):
        return pltpu.make_async_remote_copy(
            src_ref=source, dst_ref=target, send_sem=send_sem.at[to_owner], recv_sem=b_recv.at[row],
            device_id=owner, device_id_type=pl.DeviceIdType.MESH,
        )

    @pl.when(row != height)
    def _():
        to_block(own_b, blocks_b.at[row]).start()

    pass_on(PASSED_OF_16[1], 16)
    for copy in copies_s:
        copy.wait_recv()
    sums_t[col] = jnp.sum(sums_f[...], axis=0)
    copies_s = [
        sender.start(sums_t.at[col], sums_t.at[col], {"fs": row, "tp": lax.rem(col + o, nt)})
        for o in range(1, nt)
    ]

    def spread_copy(o):
        return pltpu.make_async_remote_copy(
            src_ref=blocks_b, dst_ref=blocks_b, send_sem=send_sem.at[spread + o - 1], recv_sem=b_recv.at[nf],
            device_id=above(o), device_id_type=pl.DeviceIdType.MESH,
        )

    @pl.when(row == height)
    def _():
        blocks_b[row] = own_b[...]
        for o in range(1, nf):
            source = lax.rem(row + o, nf)
            pltpu.make_async_remote_copy(
                src_ref=own_b, dst_ref=blocks_b.at[source], send_sem=send_sem.at[to_owner],
                recv_sem=b_recv.at[source], device_id=owner, device_id_type=pl.DeviceIdType.MESH,
            ).wait_recv()
        for o in range(1, nz):
            spread_copy(o).start()

    for copy in copies_qk:
        copy.wait_recv()
    need("qf", "qs", "kf", "ks", "qb", "kb", "mk")
    if early < rows_in:
        need("mq2")
    for copy in copies_s:
        copy.wait_recv()
    total = jnp.sum(sums_t[...], axis=0)[0:1, 0:1]
    entries = rank * nt * (2 * query_cols + key_cols)
    clip = 1.0 / jnp.maximum(1.0, jnp.sqrt(total / float(entries)) / CLIP_RMS)

    query_low, key_low = take_qk(all_qk[...].reshape(rank, cols + 128))
    qf_out[...], qs_out[...], q_dir = moments(qf_ref[...], qs_ref[...], query_low, clip)
    kf_out[...], ks_out[...], k_dir = moments(kf_ref[...], ks_ref[...], key_low, clip)
    q_terms, k_terms = split_two(q_dir), split_two(k_dir)
    late = []

    def send_block(out, base, count):
        part_rows = count // 2
        for h in range(2):
            target = pl.ds(base + h * part_rows, part_rows)
            for n in ((0, 1), (1, 0))[h]:
                held = out.at[row, target]
                late.append((n, h, out, target, sender.start(held, held, names[n])))

    def basis_rows(ref, source, base, count):
        return ref[pl.ds(pl.multiple_of(source * rows_in + base, 16), count), :]

    def own_update(step_ref, new_ref, out, master, basis, terms, base, count):
        rows = slice(base, base + count)
        step = exact_dot(basis_rows(basis, row, base, count), terms)
        step_ref[rows, :] = step
        updated = master[rows, :] - LEARN * step
        new_ref[rows, :] = updated
        out[row, rows, :] = updated.astype(out.dtype)

    if early < rows_in:
        own_update(q_step, q_new, q_out, mq_ref, qb_ref, q_terms, early, rows_in - early)
        send_block(q_out, early, rows_in - early)
    own_update(k_step, k_new, k_out, mk_ref, kb_ref, k_terms, 0, rows_in)
    send_block(k_out, 0, rows_in)

    @pl.when(row != height)
    def _():
        spread_copy(1).wait_recv()

    swap_b = sender.start(blocks_b, pair_b, pair)
    need("bf", "bs", "mb")
    swap_b.wait_recv()

    def branch_low(held):
        return [unpack_columns(held[n, :wide, :], held[n, wide:, :]) for n in range(nf)]

    mine, theirs = branch_low(blocks_b), branch_low(pair_b)
    for place in range(2):
        here = core == place
        for n in range(nf):
            low = jnp.where(here, mine[n], theirs[n])
            rows = slice(place * features + n * wide, place * features + (n + 1) * wide)
            bf_out[rows, :], bs_out[rows, :], b_dir = moments(bf_ref[rows, :], bs_ref[rows, :], low, clip)
            step = sum(
                jnp.dot(term, bbt_ref[...], preferred_element_type=jnp.float32)
                for term in split_two(b_dir)
            )
            b_step[rows, :] = step
            updated = mb_ref[rows, :] - LEARN * step
            b_new[rows, :] = updated
            b_out[row, rows, :] = updated.astype(b_out.dtype)
    send_block(b_out, 0, rows_in)

    own_update(q_step, q_new, q_out, mq_ref, qb_ref, q_terms, 0, early)
    for copy in sent[2:] + passed:
        copy.wait_recv()
    for o in range(1, nf):
        source = lax.rem(row + o, nf)
        step = exact_dot(basis_rows(qb_ref, source, 0, early), q_terms)
        master = decoded(far[source], MASTER_POWER) * (1.0 / MASTER_GAIN)
        q_out[source, :early, :] = (master - LEARN * step).astype(q_out.dtype)

    last = []
    for n, h, out, target, copy in late:
        copy.wait_recv()
        if n == h:
            held = out.at[(side, front)[n], target]
            last.append(sender.start(held, held, names[1 - n]))
    for copy in last:
        copy.wait_recv()
    sender.drain()

    @pl.when(row != height)
    def _():
        to_block(own_b, blocks_b.at[row]).wait_send()

    @pl.when(row == height)
    def _():
        for o in range(1, nz):
            spread_copy(o).wait_send()


def flush_kernel(*refs):
    count = len(refs) // 2
    copies = []
    for n in range(count):
        copies.append(pltpu.make_async_copy(refs[n], refs[count + n], refs[-1].at[n]))
        copies[-1].start()
    for copy in copies:
        copy.wait()


def flushed(results):
    return pl.pallas_call(
        flush_kernel,
        out_shape=tuple(jax.ShapeDtypeStruct(r.shape, r.dtype) for r in results),
        in_specs=[pl.BlockSpec(memory_space=pltpu.VMEM)] * len(results),
        out_specs=(pl.BlockSpec(memory_space=pl.ANY),) * len(results),
        scratch_shapes=[pltpu.SemaphoreType.DMA((len(results),))],
        compiler_params=pltpu.CompilerParams(vmem_limit_bytes=2**20),
    )(*results)


def fused(nf, nt, early, *args):
    x, qu, ku, h, bu, mq, mk, mb, qb, kb, bb, qf, qs, kf, ks, bf, bs = args
    tokens, features = x.shape
    rank = qb.shape[1]
    half, nz = tokens // 2, nt // 2
    piece, thin, wide = half // nz, rank // nf, features // nf
    cols = qu.shape[1] + ku.shape[1]
    coded_rows = 3 * rank + 16
    count = 80
    f32, b16 = jnp.float32, jnp.bfloat16
    vmem = pltpu.VMEM
    outs = [vmem(m.shape, f32) for m in (mq, mk, mb)] * 2
    outs += [vmem((nf, *m.shape), b16) for m in (mq, mk, mb)]
    outs += [vmem(m.shape, f32) for m in (qf, qs, kf, ks, bf, bs)]
    held = (x, qu, ku, h, bu, mq, mk, mb, qb, kb, qf, qs, kf, ks, bf, bs)
    results = pl.pallas_call(
        functools.partial(fused_kernel, nf, nt, early),
        out_shape=tuple(outs),
        in_specs=[pl.BlockSpec(memory_space=pl.ANY)] * len(args),
        out_specs=(pl.BlockSpec(memory_space=pltpu.VMEM),) * len(outs),
        scratch_shapes=[
            *[vmem(a.shape, a.dtype) for a in held],
            vmem((3, features, rank), b16),
            vmem((3 * rank, features), b16),
            vmem((rank, features), b16),
            vmem((3 * rank, half), f32),
            vmem((3 * rank, half), f32),
            vmem((nz, 3 * rank, piece), f32),
            vmem((nz, coded_rows, piece), b16),
            vmem((nz - 1, coded_rows, piece), b16),
            vmem((nz, coded_rows, piece), b16),
            vmem((nz, coded_rows, piece), b16),
            vmem((3, 2 * rank, half), b16),
            vmem((nf, thin, cols), f32),
            vmem((nf, rank, wide), f32),
            vmem((nf, thin, cols + 128), b16),
            vmem((nf, rank + 16, wide), b16),
            vmem((nf - 1, thin, cols + 128), b16),
            vmem((nf - 1, rank + 16, wide), b16),
            vmem((nf, thin, cols + 128), b16),
            vmem((wide + 16, rank), b16),
            vmem((nf, wide + 16, rank), b16),
            vmem((nf, wide + 16, rank), b16),
            vmem((nf, 8, 128), f32),
            vmem((nt, 8, 128), f32),
            vmem((early, mq.shape[1]), b16),
            vmem((nf, early, mq.shape[1]), b16),
            pltpu.SemaphoreType.DMA((count,)),
            pltpu.SemaphoreType.DMA((count,)),
            pltpu.SemaphoreType.DMA((32,)),
            pltpu.SemaphoreType.DMA((nf + 1,)),
        ],
        compiler_params=pltpu.CompilerParams(
            collective_id=0, has_side_effects=True, vmem_limit_bytes=VMEM_LIMIT
        ),
    )(*args)
    results = list(flushed(results))
    results[6:9] = [r.reshape(-1, r.shape[-1]) for r in results[6:9]]
    return tuple(results)


def per_device(
    normed_inputs,
    query_upstream,
    key_upstream,
    head_outputs,
    branch_upstream,
    query_master,
    key_master,
    branch_master,
    query_basis,
    key_basis,
    branch_basis,
    query_first,
    query_second,
    key_first,
    key_second,
    branch_first,
    branch_second,
):
    exact = lax.Precision.HIGHEST
    row_index = lax.axis_index("fs")
    col_index = lax.axis_index("tp")
    n_rows = lax.axis_size("fs")
    n_cols = lax.axis_size("tp")
    features = normed_inputs.shape[1]
    query_local = query_upstream.shape[1]
    key_local = key_upstream.shape[1]
    rows_in = query_master.shape[0]
    rank = query_basis.shape[1]
    even = n_cols == 2 * n_rows and features * 2 == rows_in and key_local % 128 == 0
    if n_rows == 4 and even and features % 512 == 0 and normed_inputs.shape[0] % 1024 == 0:
        return fused(
            n_rows, n_cols, rows_in // 64 * EARLY_OF_64, normed_inputs, query_upstream, key_upstream,
            head_outputs, branch_upstream, query_master, key_master, branch_master,
            query_basis, key_basis, branch_basis, query_first, query_second,
            key_first, key_second, branch_first, branch_second,
        )

    def own_block(basis):
        return lax.dynamic_slice_in_dim(basis, col_index * features, features, 0)

    block_branch = own_block(branch_basis)
    own_branch = block_branch.astype(jnp.float32)
    lanes = -key_local % 128
    early = rows_in // 32 * 20
    low, branch_low, squares, far = reduced(
        n_rows,
        n_cols,
        early,
        normed_inputs,
        query_upstream,
        jnp.pad(key_upstream, ((0, 0), (0, lanes))),
        head_outputs,
        branch_upstream,
        query_master,
        own_block(query_basis),
        own_block(key_basis),
        block_branch,
    )
    query_low = low[:, :query_local]
    key_low = low[:, query_local : query_local + key_local]
    branch_low = branch_low.reshape(branch_first.shape)
    total = squares[0, 0]
    entries = rank * n_cols * (2 * query_local + key_local)
    rms_value = jnp.sqrt(total / float(entries))
    clip = 1.0 / jnp.maximum(1.0, rms_value / CLIP_RMS)
    q_first, q_second, q_dir = moments(query_first, query_second, query_low, clip)
    k_first, k_second, k_dir = moments(key_first, key_second, key_low, clip)
    b_first, b_second, b_dir = moments(branch_first, branch_second, branch_low, clip)
    step_rows_query = lax.dynamic_slice_in_dim(query_basis, row_index * rows_in, rows_in, 0).astype(
        jnp.float32
    )
    step_rows_key = lax.dynamic_slice_in_dim(key_basis, row_index * rows_in, rows_in, 0).astype(
        jnp.float32
    )
    query_step = jnp.dot(step_rows_query, q_dir, precision=exact)
    key_step = jnp.dot(step_rows_key, k_dir, precision=exact)
    branch_step = jnp.dot(b_dir, own_branch.T, precision=exact)
    query_updated = query_master - LEARN * query_step
    key_updated = key_master - LEARN * key_step
    branch_updated = branch_master - LEARN * branch_step
    query_copy, branch_copy, key_copy = gathered_rows(
        n_rows,
        n_cols,
        query_updated[early:].astype(jnp.bfloat16),
        branch_updated.astype(jnp.bfloat16),
        jnp.pad(key_updated, ((0, 0), (0, lanes))).astype(jnp.bfloat16),
        far,
        query_master,
        query_basis,
        q_dir,
    )
    key_copy = key_copy[:, :key_local]
    return (
        query_step,
        key_step,
        branch_step,
        query_updated,
        key_updated,
        branch_updated,
        query_copy,
        key_copy,
        branch_copy,
        q_first,
        q_second,
        k_first,
        k_second,
        b_first,
        b_second,
    )


def solution(mesh):
    return jax.shard_map(
        per_device,
        mesh=mesh,
        in_specs=(
            P("fs", "tp"),
            P("fs", "tp"),
            P("fs", "tp"),
            P("fs", "tp"),
            P("fs", "tp"),
            P("fs", "tp"),
            P("fs", "tp"),
            P("fs", "tp"),
            P(),
            P(),
            P(),
            P(None, "tp"),
            P(None, "tp"),
            P(None, "tp"),
            P(None, "tp"),
            P("fs", None),
            P("fs", None),
        ),
        out_specs=(
            P("fs", "tp"),
            P("fs", "tp"),
            P("fs", "tp"),
            P("fs", "tp"),
            P("fs", "tp"),
            P("fs", "tp"),
            P(None, "tp"),
            P(None, "tp"),
            P(None, "tp"),
            P(None, "tp"),
            P(None, "tp"),
            P(None, "tp"),
            P(None, "tp"),
            P("fs", None),
            P("fs", None),
        ),
        check_vma=False,
    )
```

```python
import functools

import jax
import jax.numpy as jnp
from jax import lax
from jax.experimental import pallas as pl
from jax.experimental.pallas import tpu as pltpu
from jax.sharding import PartitionSpec as P

LEARN = 0.02
BETA_ONE = 0.9
BETA_TWO = 0.95
ADAM_EPS = 1e-08
CLIP_RMS = 0.5


def moments(first, second, low, clip):
    scaled = clip * low
    first_new = BETA_ONE * first + (1.0 - BETA_ONE) * scaled
    second_new = BETA_TWO * second + (1.0 - BETA_TWO) * scaled * scaled
    return (first_new, second_new, first_new / (jnp.sqrt(second_new) + ADAM_EPS))


def over_tokens(left, right, precision=None):
    return lax.dot_general(
        left,
        right,
        (((0,), (0,)), ((), ())),
        precision=precision,
        preferred_element_type=jnp.float32,
    )


def split_three(values):
    high = values.astype(jnp.bfloat16)
    rest = values - high.astype(jnp.float32)
    middle = rest.astype(jnp.bfloat16)
    low = (rest - middle.astype(jnp.float32)).astype(jnp.bfloat16)
    return high, middle, low


class Sender:
    def __init__(self, send_sem, recv_sem):
        self.send_sem, self.recv_sem, self.used, self.started = send_sem, recv_sem, 0, []

    def reserve(self, count):
        self.used += count
        return self.used - count

    def start(self, source, target, device):
        copy = pltpu.make_async_remote_copy(
            src_ref=source,
            dst_ref=target,
            send_sem=self.send_sem.at[self.used],
            recv_sem=self.recv_sem.at[self.used],
            device_id=device,
            device_id_type=pl.DeviceIdType.MESH,
        )
        self.used += 1
        copy.start()
        self.started.append(copy)
        return copy

    def drain(self):
        for copy in self.started:
            copy.wait_send()


def greet(nf, nt, row, col, both):
    barrier = pltpu.get_barrier_semaphore()
    peers = [{"fs": lax.rem(row + o, nf), "tp": col} for o in range(1, nf)]
    if both:
        peers += [{"fs": row, "tp": lax.rem(col + o, nt)} for o in range(1, nt)]
    for peer in peers:
        pl.semaphore_signal(
            barrier, inc=1, device_id=peer, device_id_type=pl.DeviceIdType.MESH
        )
    pl.semaphore_wait(barrier, len(peers))


def square(row, col):
    side = row + 1 - 2 * lax.rem(row, 2)
    front = lax.rem(row + 2, 4)
    return side, front, ({"fs": side, "tp": col}, {"fs": front, "tp": col})


def reduce_kernel(
    nf, nt,
    x_hbm, qu_hbm, ku_hbm, h_hbm, bu_hbm, master_ref, qb_ref, kb_ref, bb_ref,
    qk_out, b_out, total_out, far_out,
    x_ref, qu_ref, ku_ref, h_ref, bu_ref,
    part, from_pair, halves, arrived, whole, other,
    part_qk, part_b, got_qk, got_b, all_qk, all_b, spread_b, sums,
    send_sem, recv_sem, load_sem,
):
    row, col = lax.axis_index("fs"), lax.axis_index("tp")
    core, height = lax.rem(col, 2), lax.div(col, 2)
    nz = nt // 2
    rank = qb_ref.shape[1]
    half = x_ref.shape[0] // 2
    piece = half // nz
    query_cols = qu_ref.shape[1]
    loads = []

    def load(source, target):
        copy = pltpu.make_async_copy(source, target, load_sem.at[len(loads)])
        copy.start()
        loads.append(copy)

    for which in (1 - core, core):
        rows = pl.ds(pl.multiple_of(which * half, half), half)
        load(x_hbm.at[rows], x_ref.at[rows])
        load(bu_hbm.at[rows], bu_ref.at[rows])
    load(qu_hbm, qu_ref)
    load(ku_hbm, ku_ref)
    load(h_hbm, h_ref)
    greet(nf, nt, row, col, True)
    sender = Sender(send_sem, recv_sem)
    pair = {"fs": row, "tp": height * 2 + (1 - core)}

    def above(o):
        return {"fs": row, "tp": lax.rem(height + o, nz) * 2 + core}

    def beside(o):
        return {"fs": lax.rem(row + o, nf), "tp": col}

    def project(which):
        rows = pl.ds(pl.multiple_of(which * half, half), half)
        x = x_ref[rows, :]
        return (
            jnp.dot(x, qb_ref[...], preferred_element_type=jnp.float32),
            jnp.dot(x, kb_ref[...], preferred_element_type=jnp.float32),
            jnp.dot(bu_ref[rows, :], bb_ref[...], preferred_element_type=jnp.float32),
        )

    early = far_out.shape[1]
    sent = []
    if nf == 4:
        side, front, names = square(row, col)
        for turn in range(2):
            for n in range(2):
                rows = pl.ds((turn ^ n) * (early // 2), early // 2)
                sent.append(
                    sender.start(master_ref.at[rows], far_out.at[row, rows], names[n])
                )
    else:
        rows = pl.ds(0, early)
        for o in range(1, nf):
            sent.append(sender.start(master_ref.at[rows], far_out.at[row], beside(o)))
    loads[0].wait()
    loads[1].wait()
    for n, value in enumerate(project(1 - core)):
        part[:, n * rank : (n + 1) * rank] = value
    swap = sender.start(part, from_pair, pair)
    loads[2].wait()
    loads[3].wait()
    own = project(core)
    swap.wait_recv()
    for n, value in enumerate(own):
        span = slice(n * rank, (n + 1) * rank)
        halves[:, :, span] = (value + from_pair[:, span]).reshape(nz, piece, rank)
    copies = [
        sender.start(halves.at[lax.rem(height + o, nz)], arrived.at[o - 1], above(o))
        for o in range(1, nz)
    ]
    total = halves[height]
    for o, copy in enumerate(copies):
        copy.wait_recv()
        total = total + arrived[o]
    whole[height] = total
    copies = [sender.start(whole.at[height], whole.at[height], above(o)) for o in range(1, nz)]
    across = [sender.start(whole.at[height], other.at[height], pair)]
    passed = []
    if nf == 4:
        for n, source in ((0, side), (1, front)):
            sent[n].wait_recv()
            held = far_out.at[source, pl.ds(n * (early // 2), early // 2)]
            passed.append(sender.start(held, held, names[1 - n]))
    for o, copy in enumerate(copies, 1):
        copy.wait_recv()
        source = lax.rem(height + nz - o, nz)
        across.append(sender.start(whole.at[source], other.at[source], pair))

    over_rows = (((0,), (0,)), ((), ()))

    def low_parts(values, which):
        rows = pl.ds(pl.multiple_of(which * half, half), half)
        sides = (qu_ref[rows, :], ku_ref[rows, :], h_ref[rows, :])
        parts = []
        for n, side in enumerate(sides):
            terms = split_three(values[:, n * rank : (n + 1) * rank])
            parts.append(
                sum(
                    lax.dot_general(term, side, over_rows, preferred_element_type=jnp.float32)
                    for term in terms
                )
            )
        return parts

    for copy in loads[4:]:
        copy.wait()
    first = low_parts(whole[...].reshape(half, 3 * rank), core)
    for copy in across:
        copy.wait_recv()
    second = low_parts(other[...].reshape(half, 3 * rank), 1 - core)
    query_part, key_part, branch_part = [a + b for a, b in zip(first, second)]
    part_qk[:, :, :query_cols] = query_part.reshape(nf, rank // nf, query_cols)
    part_qk[:, :, query_cols:] = key_part.reshape(nf, rank // nf, key_part.shape[1])
    part_b[...] = branch_part.T.reshape(part_b.shape)

    copies = []
    for o in range(1, nf):
        to = lax.rem(row + o, nf)
        copies.append(sender.start(part_qk.at[to], got_qk.at[o - 1], beside(o)))
        copies.append(sender.start(part_b.at[to], got_b.at[o - 1], beside(o)))
    for copy in copies:
        copy.wait_recv()
    sum_qk, sum_b = part_qk[row], part_b[row]
    for o in range(nf - 1):
        sum_qk = sum_qk + got_qk[o]
        sum_b = sum_b + got_b[o]
    rows_b = sum_b.shape[0]
    squares = jnp.sum(sum_qk * sum_qk) + jnp.sum(sum_b * sum_b)
    all_qk[row] = sum_qk
    all_b[col, :rows_b, :] = sum_b
    all_b[col, rows_b:, :] = jnp.full((8, rank), squares, jnp.float32)

    copies_b = [
        sender.start(all_b.at[col], all_b.at[col], {"fs": row, "tp": lax.rem(col + o, nt)})
        for o in range(1, nt)
    ]
    copies_qk = [sender.start(all_qk.at[row], all_qk.at[row], beside(o)) for o in range(1, nf)]
    for copy in copies_b:
        copy.wait_recv()
    sums[row] = jnp.sum(all_b[:, rows_b:, :], axis=0)
    each = nt // nf
    copies = []
    for o in range(1, nf):
        blocks = pl.ds(lax.rem(row + o, nf) * each, each)
        copies.append(sender.start(sums.at[row], sums.at[row], beside(o)))
        copies.append(sender.start(all_b.at[blocks], spread_b.at[row], beside(o)))
    b_out[:, row] = all_b[pl.ds(row * each, each)][:, :rows_b, :]
    for copy in copies_qk:
        copy.wait_recv()
    qk_out[...] = all_qk[...].reshape(qk_out.shape)
    for copy in copies:
        copy.wait_recv()
    for o in range(1, nf):
        source = lax.rem(row + o, nf)
        b_out[:, source] = spread_b[source][:, :rows_b, :]
    total_out[...] = jnp.sum(sums[...], axis=0)
    for copy in (sent[2:] + passed) if nf == 4 else sent:
        copy.wait_recv()
    sender.drain()


def reduced(nf, nt, early, x, qu, ku, h, bu, master, qb, kb, bb):
    tokens, features = x.shape
    rank = qb.shape[1]
    cols = qu.shape[1] + ku.shape[1]
    half, nz, each = tokens // 2, nt // 2, nt // nf
    piece, thin, rows_b = half // nz, rank // nf, features // nf
    copies = 1 + 2 * (nz - 1) + nz + 2 * (nf - 1) + (nt - 1) + 3 * (nf - 1)
    copies += 6 if nf == 4 else nf - 1
    any_place = pl.BlockSpec(memory_space=pl.ANY)
    vmem = pl.BlockSpec(memory_space=pltpu.VMEM)
    f32 = jnp.float32
    return pl.pallas_call(
        functools.partial(reduce_kernel, nf, nt),
        out_shape=(
            jax.ShapeDtypeStruct((rank, cols), f32),
            jax.ShapeDtypeStruct((each, nf, rows_b, rank), f32),
            jax.ShapeDtypeStruct((8, rank), f32),
            jax.ShapeDtypeStruct((nf, early, master.shape[1]), f32),
        ),
        in_specs=[any_place] * 6 + [vmem] * 3,
        out_specs=(vmem, vmem, vmem, any_place),
        scratch_shapes=[
            *[pltpu.VMEM(each_in.shape, each_in.dtype) for each_in in (x, qu, ku, h, bu)],
            pltpu.VMEM((half, 3 * rank), f32),
            pltpu.VMEM((half, 3 * rank), f32),
            pltpu.VMEM((nz, piece, 3 * rank), f32),
            pltpu.VMEM((nz - 1, piece, 3 * rank), f32),
            pltpu.VMEM((nz, piece, 3 * rank), f32),
            pltpu.VMEM((nz, piece, 3 * rank), f32),
            pltpu.VMEM((nf, thin, cols), f32),
            pltpu.VMEM((nf, rows_b, rank), f32),
            pltpu.VMEM((nf - 1, thin, cols), f32),
            pltpu.VMEM((nf - 1, rows_b, rank), f32),
            pltpu.VMEM((nf, thin, cols), f32),
            pltpu.VMEM((nt, rows_b + 8, rank), f32),
            pltpu.VMEM((nf, each, rows_b + 8, rank), f32),
            pltpu.VMEM((nf, 8, rank), f32),
            pltpu.SemaphoreType.DMA((copies,)),
            pltpu.SemaphoreType.DMA((copies,)),
            pltpu.SemaphoreType.DMA((7,)),
        ],
        compiler_params=pltpu.CompilerParams(
            collective_id=0, has_side_effects=True, vmem_limit_bytes=58 * 2**20
        ),
    )(x, qu, ku, h, bu, master, qb, kb, bb)


def gather_kernel(
    nf, nt,
    q_ref, b_ref, k_ref, far_ref, master_ref, basis_ref, dir_ref,
    q_out, b_out, k_out,
    held_far, held_copy, send_sem, recv_sem, own_sem, load_sem, store_sem,
):
    row, col = lax.axis_index("fs"), lax.axis_index("tp")
    early = far_ref.shape[1]
    pairs = ((q_ref, q_out, early), (b_ref, b_out, 0), (k_ref, k_out, 0))

    def load(o):
        source = master_ref.at[pl.ds(0, early)] if o == 0 else far_ref.at[lax.rem(row + o, nf)]
        copy = pltpu.make_async_copy(source, held_far.at[o % 2], load_sem.at[o])
        copy.start()
        return copy

    coming = load(0)
    greet(nf, nt, row, col, False)
    sender = Sender(send_sem, recv_sem)
    sent = []
    if nf == 4:
        side, front, names = square(row, col)
        for ref, out, base in pairs:
            half = ref.shape[0] // 2
            for h in range(2):
                rows = pl.ds(h * half, half)
                target = pl.ds(base + h * half, half)
                for n in ((0, 1), (1, 0))[h]:
                    copy = sender.start(ref.at[rows], out.at[row, target], names[n])
                    sent.append((n, h, out, target, copy))
    else:
        for ref, out, base in pairs:
            for o in range(1, nf):
                target = out.at[row, pl.ds(base, ref.shape[0])]
                there = {"fs": lax.rem(row + o, nf), "tp": col}
                sent.append(sender.start(ref, target, there))
    local = []
    for n, (ref, out, base) in enumerate(pairs):
        target = out.at[row, pl.ds(base, ref.shape[0])]
        local.append(pltpu.make_async_copy(ref, target, own_sem.at[n]))
        local[-1].start()

    terms = split_three(dir_ref[...])
    rows_all = q_out.shape[1]
    stores = []
    for o in range(nf):
        source = lax.rem(row + o, nf)
        coming.wait()
        if o + 1 < nf:
            coming = load(o + 1)
        if o >= 2:
            stores[o - 2].wait()
        basis = basis_ref[pl.ds(pl.multiple_of(source * rows_all, rows_all), early), :]
        step = sum(jnp.dot(basis, term, preferred_element_type=jnp.float32) for term in terms)
        held_copy[o % 2] = (held_far[o % 2] - LEARN * step).astype(held_copy.dtype)
        stores.append(
            pltpu.make_async_copy(
                held_copy.at[o % 2], q_out.at[source, pl.ds(0, early)], store_sem.at[o]
            )
        )
        stores[-1].start()

    if nf == 4:
        last = []
        for n, h, out, target, copy in sent:
            copy.wait_recv()
            if n == h:
                held = out.at[(side, front)[n], target]
                last.append(sender.start(held, held, names[1 - n]))
        sent = last
    for copy in sent:
        copy.wait_recv()
    for copy in local + stores[-2:]:
        copy.wait()
    sender.drain()


def gathered_rows(nf, nt, q_tail, b_block, k_block, far, master, basis, direction):
    count = 18 if nf == 4 else 3 * (nf - 1)
    early = far.shape[1]
    blocks = (master, b_block, k_block)
    wide = [jax.ShapeDtypeStruct((nf, *block.shape), q_tail.dtype) for block in blocks]
    vmem = pl.BlockSpec(memory_space=pltpu.VMEM)
    any_place = pl.BlockSpec(memory_space=pl.ANY)
    outs = pl.pallas_call(
        functools.partial(gather_kernel, nf, nt),
        out_shape=tuple(wide),
        in_specs=[vmem] * 3 + [any_place] * 2 + [vmem] * 2,
        out_specs=(any_place,) * 3,
        scratch_shapes=[
            pltpu.VMEM((2, early, far.shape[2]), far.dtype),
            pltpu.VMEM((2, early, far.shape[2]), q_tail.dtype),
            pltpu.SemaphoreType.DMA((count,)),
            pltpu.SemaphoreType.DMA((count,)),
            pltpu.SemaphoreType.DMA((3,)),
            pltpu.SemaphoreType.DMA((nf,)),
            pltpu.SemaphoreType.DMA((nf,)),
        ],
        compiler_params=pltpu.CompilerParams(
            collective_id=1, has_side_effects=True, vmem_limit_bytes=48 * 2**20
        ),
    )(q_tail, b_block, k_block, far, master, basis, direction)
    return [out.reshape(-1, out.shape[-1]) for out in outs]


EARLY_OF_64 = 64
PASSED_OF_16 = (9, 11)
K_EARLY_OF_16 = 16
KEY_LATER = False
VMEM_LIMIT = 40 * 2**20
MASTER_MOST = 0.09375
MASTER_POWER = 14
MASTER_GAIN = 515.0 / MASTER_MOST
SUM_POWER = 16
SUM_GAIN = 238.0


def raised(magnitude, power):
    result, square = None, magnitude
    while power:
        if power % 2:
            result = square if result is None else result * square
        power //= 2
        if power:
            square = square * square
    return result


def coded(values, power):
    high = raised(jnp.abs(values), power)
    return jnp.where(values < 0, -high, high).astype(jnp.bfloat16)


def decoded(codes, power):
    codes = codes.astype(jnp.float32)
    root = jnp.exp(jnp.log(jnp.abs(codes)) * (1.0 / power))
    root = jnp.where(codes == 0, 0.0, root)
    return jnp.where(codes < 0, -root, root)


def pack(values, axis):
    most = jnp.max(jnp.abs(values), axis=axis, keepdims=True)
    scale = jnp.maximum(most, 1e-30).astype(jnp.bfloat16).astype(jnp.float32)
    return coded(values * (SUM_GAIN / scale), SUM_POWER), scale


def unpack(codes, scale):
    return decoded(codes, SUM_POWER) * (scale.astype(jnp.float32) * (1.0 / SUM_GAIN))


def pack_columns(values):
    codes, scale = pack(values, 0)
    return codes, jnp.broadcast_to(scale, (16, values.shape[1])).astype(jnp.bfloat16)


def unpack_columns(codes, scale):
    return unpack(codes, scale[0:1])


def stacked(scales, width):
    place = lax.broadcasted_iota(jnp.int32, (16, width), 0)
    rows = jnp.broadcast_to(scales[-1], (16, width))
    for n, scale in enumerate(scales[:-1]):
        rows = jnp.where(place == n, scale, rows)
    return rows.astype(jnp.bfloat16)


def split_two(values):
    high = values.astype(jnp.bfloat16)
    return high, (values - high.astype(jnp.float32)).astype(jnp.bfloat16)


def exact_dot(left, terms):
    return sum(jnp.dot(left, term, preferred_element_type=jnp.float32) for term in terms)


def fused_kernel(
    nf, nt, early,
    x_hbm, qu_hbm, ku_hbm, h_hbm, bu_hbm, mq_hbm, mk_hbm, mb_hbm, qb_hbm, kb_hbm, bb_hbm,
    qf_hbm, qs_hbm, kf_hbm, ks_hbm, bf_hbm, bs_hbm,
    q_step, k_step, b_step, q_new, k_new, b_new, q_out, k_out, b_out,
    qf_out, qs_out, kf_out, ks_out, bf_out, bs_out,
    x_ref, qu_ref, ku_ref, h_ref, bu_ref, mq_ref, mk_ref, mb_ref, qb_ref, kb_ref,
    qf_ref, qs_ref, kf_ref, ks_ref, bf_ref, bs_ref, own_ref, turned, bbt_ref,
    part, from_pair, halves, sent_z, arrived, whole, other, split_ref,
    part_qk, part_b, sent_qk, sent_b, got_qk, got_b, all_qk, own_b, blocks_b, pair_b, sums_f, sums_t,
    enc, far, enc_k, far_k,
    send_sem, recv_sem, load_sem, b_recv,
):
    row, col = lax.axis_index("fs"), lax.axis_index("tp")
    core, height = lax.rem(col, 2), lax.div(col, 2)
    nz = nt // 2
    rank = qb_ref.shape[1]
    tokens, features = x_ref.shape
    half = tokens // 2
    piece = half // nz
    query_cols, key_cols = qu_ref.shape[1], ku_ref.shape[1]
    rows_in = mq_ref.shape[0]
    loads = {}
    barrier = pltpu.get_barrier_semaphore()
    peers = [{"fs": lax.rem(row + o, nf), "tp": col} for o in range(1, nf)]
    peers += [{"fs": row, "tp": lax.rem(col + o, nt)} for o in range(1, nt)]
    for peer in peers:
        pl.semaphore_signal(barrier, inc=1, device_id=peer, device_id_type=pl.DeviceIdType.MESH)

    def load(name, source, target):
        copy = pltpu.make_async_copy(source, target, load_sem.at[len(loads)])
        copy.start()
        loads[name] = copy

    needed = set()

    def need(*keys):
        for key in keys:
            if key not in needed:
                needed.add(key)
                loads[key].wait()

    def token_rows(which):
        return pl.ds(pl.multiple_of(which * half, half), half)

    k_early = enc_k.shape[0]
    first, second = pl.ds(0, early // 2), pl.ds(early // 2, early // 2)
    load("mq0", mq_hbm.at[first], mq_ref.at[first])
    load("mq1", mq_hbm.at[second], mq_ref.at[second])
    own_rows = pl.ds(pl.multiple_of(col * features, features), features)
    for n, basis in enumerate((qb_hbm, kb_hbm, bb_hbm)):
        load(("own", n), basis.at[own_rows], own_ref.at[n])
    for n, which in enumerate((1 - core, core)):
        load(("x", n), x_hbm.at[token_rows(which)], x_ref.at[token_rows(which)])
        load(("bu", n), bu_hbm.at[token_rows(which)], bu_ref.at[token_rows(which)])
    load("qu", qu_hbm, qu_ref)
    load("ku", ku_hbm, ku_ref)
    load("h", h_hbm, h_ref)
    if early < rows_in:
        rest = pl.ds(early, rows_in - early)
        load("mq2", mq_hbm.at[rest], mq_ref.at[rest])
    for name, source, target in (
        ("qf", qf_hbm, qf_ref), ("qs", qs_hbm, qs_ref), ("kf", kf_hbm, kf_ref), ("ks", ks_hbm, ks_ref),
        ("qb", qb_hbm, qb_ref), ("kb", kb_hbm, kb_ref), ("mk", mk_hbm, mk_ref),
        ("bf", bf_hbm, bf_ref), ("bs", bs_hbm, bs_ref), ("mb", mb_hbm, mb_ref),
    ):
        load(name, source, target)

    sender = Sender(send_sem, recv_sem)
    pair = {"fs": row, "tp": height * 2 + (1 - core)}
    side, front, names = square(row, col)

    def above(o):
        return {"fs": row, "tp": lax.rem(height + o, nz) * 2 + core}

    def beside(o):
        return {"fs": lax.rem(row + o, nf), "tp": col}

    parts = (first, second)
    for n in range(2):
        need(f"mq{n}")
        enc[parts[n], :] = coded(mq_ref[parts[n], :] * MASTER_GAIN, MASTER_POWER)
    for n in range(3):
        need(("own", n))
        turned[n * rank : (n + 1) * rank, :] = own_ref[n].T

    def project(n, which):
        need(("x", n), ("bu", n))
        over = (((1,), (1,)), ((), ()))
        a = lax.dot_general(turned[: 2 * rank, :], x_ref[token_rows(which), :], over, preferred_element_type=jnp.float32)
        b = lax.dot_general(turned[2 * rank :, :], bu_ref[token_rows(which), :], over, preferred_element_type=jnp.float32)
        return a, b

    a, b = project(0, 1 - core)
    part[: 2 * rank, :] = a
    part[2 * rank :, :] = b
    pl.semaphore_wait(barrier, len(peers))
    sent = []
    for turn in range(2):
        for n in range(2):
            rows = parts[turn ^ n]
            sent.append(sender.start(enc.at[rows], far.at[row, rows], names[n]))
    swap = sender.start(part, from_pair, pair)
    a, b = project(1, core)
    swap.wait_recv()
    for n in range(nz):
        span = slice(n * piece, (n + 1) * piece)
        halves[n, : 2 * rank, :] = a[:, span] + from_pair[: 2 * rank, span]
        halves[n, 2 * rank :, :] = b[:, span] + from_pair[2 * rank :, span]

    def put(target, n, values):
        scales = []
        for k in range(3):
            codes, scale = pack(values[k], 0)
            target[n, k * rank : (k + 1) * rank, :] = codes
            scales.append(scale)
        target[n, 3 * rank :, :] = stacked(scales, piece)

    def take(source, n, k):
        scale = source[n, 3 * rank :, :].astype(jnp.float32)[k : k + 1]
        return unpack(source[n, k * rank : (k + 1) * rank, :], scale)

    def thirds(values):
        return [values[k * rank : (k + 1) * rank] for k in range(3)]

    copies = []
    for o in range(1, nz):
        to = lax.rem(height + o, nz)
        put(sent_z, to, thirds(halves[to]))
        copies.append(sender.start(sent_z.at[to], arrived.at[o - 1], above(o)))
    for copy in copies:
        copy.wait_recv()
    totals = thirds(halves[height])
    for k in range(3):
        for o in range(nz - 1):
            totals[k] = totals[k] + take(arrived, o, k)
    put(whole, height, totals)
    copies = [sender.start(whole.at[height], whole.at[height], above(o)) for o in range(1, nz)]
    across = [sender.start(whole.at[height], other.at[height], pair)]

    passed = []

    def pass_on(begin, end):
        if begin == end:
            return
        unit = early // 32
        for n, source in ((0, side), (1, front)):
            held = far.at[source, pl.ds(n * (early // 2) + begin * unit, (end - begin) * unit)]
            passed.append(sender.start(held, held, names[1 - n]))

    for n in range(2):
        sent[n].wait_recv()
    pass_on(0, PASSED_OF_16[0])

    bbt_ref[...] = turned[2 * rank :, :]
    for o, copy in enumerate(copies, 1):
        copy.wait_recv()
        source = lax.rem(height + nz - o, nz)
        across.append(sender.start(whole.at[source], other.at[source], pair))

    def low_parts(held, which):
        for n in range(nz):
            for k in range(3):
                high, low = split_two(take(held, n, k))
                split_ref[k, :rank, n * piece : (n + 1) * piece] = high
                split_ref[k, rank:, n * piece : (n + 1) * piece] = low
        lows = []
        for k, ref in enumerate((qu_ref, ku_ref, h_ref)):
            both = jnp.dot(split_ref[k], ref[token_rows(which), :], preferred_element_type=jnp.float32)
            lows.append(both[:rank] + both[rank:])
        return lows

    need("qu", "ku", "h")
    one = low_parts(whole, core)
    for copy in across:
        copy.wait_recv()
    two = low_parts(other, 1 - core)
    thin, wide = rank // nf, features // nf
    query_part, key_part, branch_part = [a + b for a, b in zip(one, two)]
    cols = query_cols + key_cols

    def put_qk(query, key):
        query_codes, query_scale = pack(query, 1)
        key_codes, key_scale = pack(key, 1)
        place = lax.broadcasted_iota(jnp.int32, (query.shape[0], 128), 1)
        scale = jnp.where(place < 64, query_scale, key_scale).astype(jnp.bfloat16)
        return ((slice(0, query_cols), query_codes), (slice(query_cols, cols), key_codes), (slice(cols, cols + 128), scale))

    def take_qk(held):
        scale = held[:, cols:].astype(jnp.float32)
        return unpack(held[:, :query_cols], scale[:, 0:1]), unpack(held[:, query_cols:cols], scale[:, 64:65])

    for span, values in put_qk(query_part, key_part):
        sent_qk[:, :, span] = values.reshape(nf, thin, values.shape[1])
    part_qk[:, :, :query_cols] = query_part.reshape(nf, thin, query_cols)
    part_qk[:, :, query_cols:] = key_part.reshape(nf, thin, key_cols)
    codes, scale = pack_columns(branch_part)
    for n in range(nf):
        part_b[n] = branch_part[:, n * wide : (n + 1) * wide]
        sent_b[n, :rank, :] = codes[:, n * wide : (n + 1) * wide]
        sent_b[n, rank:, :] = scale[:, n * wide : (n + 1) * wide]

    copies = []
    for o in range(1, nf):
        to = lax.rem(row + o, nf)
        copies.append(sender.start(sent_qk.at[to], got_qk.at[o - 1], beside(o)))
        copies.append(sender.start(sent_b.at[to], got_b.at[o - 1], beside(o)))
    need("mk")
    enc_k[...] = coded(mk_ref[:k_early, :] * MASTER_GAIN, MASTER_POWER)
    sent_k = []

    def send_key():
        for h in range(2):
            rows = pl.ds(h * (k_early // 2), k_early // 2)
            for n in ((0, 1), (1, 0))[h]:
                copy = sender.start(enc_k.at[rows], far_k.at[row, rows], names[n])
                sent_k.append((n, h, rows, copy))

    def pass_key():
        for n, h, rows, copy in sent_k:
            copy.wait_recv()
            if n == h:
                held = far_k.at[(side, front)[n], rows]
                passed.append(sender.start(held, held, names[1 - n]))

    if not KEY_LATER:
        send_key()
    pass_on(*PASSED_OF_16)
    for copy in copies:
        copy.wait_recv()
    sum_q, sum_k, sum_b = part_qk[row, :, :query_cols], part_qk[row, :, query_cols:], part_b[row]
    for o in range(nf - 1):
        got_query, got_key = take_qk(got_qk[o])
        sum_q, sum_k = sum_q + got_query, sum_k + got_key
        sum_b = sum_b + unpack_columns(got_b[o, :rank, :], got_b[o, rank:, :])
    squares = jnp.sum(sum_q * sum_q) + jnp.sum(sum_k * sum_k) + jnp.sum(sum_b * sum_b)
    sums_f[row] = jnp.full((8, 128), squares, jnp.float32)
    copies_s = [sender.start(sums_f.at[row], sums_f.at[row], beside(o)) for o in range(1, nf)]
    for span, values in put_qk(sum_q, sum_k):
        all_qk[row, :, span] = values
    copies_qk = [sender.start(all_qk.at[row], all_qk.at[row], beside(o)) for o in range(1, nf)]
    sum_b = sum_b.T
    codes, scale = pack_columns(sum_b)
    own_b[:wide, :] = codes
    own_b[wide:, :] = scale

    spread = sender.reserve(nf * (nz - 1))
    to_owner = sender.reserve(1)
    owner = {"fs": height, "tp": col}

    def to_block(source, target):
        return pltpu.make_async_remote_copy(
            src_ref=source, dst_ref=target, send_sem=send_sem.at[to_owner], recv_sem=b_recv.at[row],
            device_id=owner, device_id_type=pl.DeviceIdType.MESH,
        )

    @pl.when(row != height)
    def _():
        to_block(own_b, blocks_b.at[row]).start()

    pass_on(PASSED_OF_16[1], 16)
    if KEY_LATER:
        send_key()
    else:
        pass_key()
    for copy in copies_s:
        copy.wait_recv()
    sums_t[col] = jnp.sum(sums_f[...], axis=0)
    copies_s = [
        sender.start(sums_t.at[col], sums_t.at[col], {"fs": row, "tp": lax.rem(col + o, nt)})
        for o in range(1, nt)
    ]

    def spread_copy(turn, o):
        held = blocks_b.at[lax.rem(row + turn, nf)]
        return pltpu.make_async_remote_copy(
            src_ref=held, dst_ref=held, send_sem=send_sem.at[spread + turn * (nz - 1) + o - 1],
            recv_sem=b_recv.at[nf + turn], device_id=above(o), device_id_type=pl.DeviceIdType.MESH,
        )

    @pl.when(row == height)
    def _():
        blocks_b[row] = own_b[...]
        for turn in range(nf):
            source = lax.rem(row + turn, nf)
            if turn:
                pltpu.make_async_remote_copy(
                    src_ref=own_b, dst_ref=blocks_b.at[source], send_sem=send_sem.at[to_owner],
                    recv_sem=b_recv.at[source], device_id=owner, device_id_type=pl.DeviceIdType.MESH,
                ).wait_recv()
            for o in range(nz - 1, 0, -1):
                spread_copy(turn, o).start()

    for copy in copies_qk:
        copy.wait_recv()
    need("qf", "qs", "kf", "ks", "qb", "kb")
    if early < rows_in:
        need("mq2")
    for copy in copies_s:
        copy.wait_recv()
    if KEY_LATER:
        pass_key()
    total = jnp.sum(sums_t[...], axis=0)[0:1, 0:1]
    entries = rank * nt * (2 * query_cols + key_cols)
    clip = 1.0 / jnp.maximum(1.0, jnp.sqrt(total / float(entries)) / CLIP_RMS)

    query_low, key_low = take_qk(all_qk[...].reshape(rank, cols + 128))
    qf_out[...], qs_out[...], q_dir = moments(qf_ref[...], qs_ref[...], query_low, clip)
    kf_out[...], ks_out[...], k_dir = moments(kf_ref[...], ks_ref[...], key_low, clip)
    q_terms, k_terms = split_two(q_dir), split_two(k_dir)
    late = []

    def send_block(out, span, count):
        part_rows = count // 2

        def target(source, h):
            return out.at[source, pl.ds(pl.multiple_of(span(source) + h * part_rows, part_rows), part_rows)]

        for h in range(2):
            for n in ((0, 1), (1, 0))[h]:
                held = target(row, h)
                late.append((n, h, target, sender.start(held, held, names[n])))

    def basis_rows(ref, source, base, count):
        return ref[pl.ds(pl.multiple_of(source * rows_in + base, 16), count), :]

    def own_update(step_ref, new_ref, out, master, basis, terms, base, count):
        rows = slice(base, base + count)
        step = exact_dot(basis_rows(basis, row, base, count), terms)
        step_ref[rows, :] = step
        updated = master[rows, :] - LEARN * step
        new_ref[rows, :] = updated
        out[row, rows, :] = updated.astype(out.dtype)

    if early < rows_in:
        own_update(q_step, q_new, q_out, mq_ref, qb_ref, q_terms, early, rows_in - early)
        send_block(q_out, lambda source: early, rows_in - early)
    if k_early < rows_in:
        own_update(k_step, k_new, k_out, mk_ref, kb_ref, k_terms, k_early, rows_in - k_early)
        send_block(k_out, lambda source: k_early, rows_in - k_early)
    need("bf", "bs", "mb")

    def branch_rows(held, place, turn):
        def span(source):
            return place * features + lax.rem(source + turn, nf) * wide

        source = lax.rem(row + turn, nf)
        rows = pl.ds(pl.multiple_of(span(row), wide), wide)
        low = unpack_columns(held[source, :wide, :], held[source, wide:, :])
        bf_out[rows, :], bs_out[rows, :], b_dir = moments(bf_ref[rows, :], bs_ref[rows, :], low, clip)
        step = sum(
            jnp.dot(term, bbt_ref[...], preferred_element_type=jnp.float32)
            for term in split_two(b_dir)
        )
        b_step[rows, :] = step
        updated = mb_ref[rows, :] - LEARN * step
        b_new[rows, :] = updated
        b_out[row, rows, :] = updated.astype(b_out.dtype)
        send_block(b_out, span, wide)

    for turn in range(nf):
        source = lax.rem(row + turn, nf)

        @pl.when(row != height)
        def _():
            spread_copy(turn, 1).wait_recv()

        swap_b = sender.start(blocks_b.at[source], pair_b.at[source], pair)
        branch_rows(blocks_b, core, turn)
        swap_b.wait_recv()
        branch_rows(pair_b, 1 - core, turn)

    own_update(k_step, k_new, k_out, mk_ref, kb_ref, k_terms, 0, k_early)
    own_update(q_step, q_new, q_out, mq_ref, qb_ref, q_terms, 0, early)
    for copy in sent[2:] + passed:
        copy.wait_recv()
    for o in range(1, nf):
        source = lax.rem(row + o, nf)
        for held, count, basis, terms, out in (
            (far_k, k_early, kb_ref, k_terms, k_out), (far, early, qb_ref, q_terms, q_out)
        ):
            step = exact_dot(basis_rows(basis, source, 0, count), terms)
            master = decoded(held[source], MASTER_POWER) * (1.0 / MASTER_GAIN)
            out[source, :count, :] = (master - LEARN * step).astype(out.dtype)

    last = []
    for n, h, target, copy in late:
        copy.wait_recv()
        if n == h:
            held = target((side, front)[n], h)
            last.append(sender.start(held, held, names[1 - n]))
    for copy in last:
        copy.wait_recv()
    sender.drain()

    @pl.when(row != height)
    def _():
        to_block(own_b, blocks_b.at[row]).wait_send()

    @pl.when(row == height)
    def _():
        for turn in range(nf):
            for o in range(1, nz):
                spread_copy(turn, o).wait_send()


def flush_kernel(*refs):
    count = len(refs) // 2
    copies = []
    for n in range(count):
        copies.append(pltpu.make_async_copy(refs[n], refs[count + n], refs[-1].at[n]))
        copies[-1].start()
    for copy in copies:
        copy.wait()


def flushed(results):
    return pl.pallas_call(
        flush_kernel,
        out_shape=tuple(jax.ShapeDtypeStruct(r.shape, r.dtype) for r in results),
        in_specs=[pl.BlockSpec(memory_space=pltpu.VMEM)] * len(results),
        out_specs=(pl.BlockSpec(memory_space=pl.ANY),) * len(results),
        scratch_shapes=[pltpu.SemaphoreType.DMA((len(results),))],
        compiler_params=pltpu.CompilerParams(vmem_limit_bytes=2**20),
    )(*results)


def fused(nf, nt, early, *args):
    x, qu, ku, h, bu, mq, mk, mb, qb, kb, bb, qf, qs, kf, ks, bf, bs = args
    tokens, features = x.shape
    rank = qb.shape[1]
    half, nz = tokens // 2, nt // 2
    piece, thin, wide = half // nz, rank // nf, features // nf
    cols = qu.shape[1] + ku.shape[1]
    coded_rows = 3 * rank + 16
    count = 136
    k_early = early // 16 * K_EARLY_OF_16
    f32, b16 = jnp.float32, jnp.bfloat16
    vmem = pltpu.VMEM
    outs = [vmem(m.shape, f32) for m in (mq, mk, mb)] * 2
    outs += [vmem((nf, *m.shape), b16) for m in (mq, mk, mb)]
    outs += [vmem(m.shape, f32) for m in (qf, qs, kf, ks, bf, bs)]
    held = (x, qu, ku, h, bu, mq, mk, mb, qb, kb, qf, qs, kf, ks, bf, bs)
    results = pl.pallas_call(
        functools.partial(fused_kernel, nf, nt, early),
        out_shape=tuple(outs),
        in_specs=[pl.BlockSpec(memory_space=pl.ANY)] * len(args),
        out_specs=(pl.BlockSpec(memory_space=pltpu.VMEM),) * len(outs),
        scratch_shapes=[
            *[vmem(a.shape, a.dtype) for a in held],
            vmem((3, features, rank), b16),
            vmem((3 * rank, features), b16),
            vmem((rank, features), b16),
            vmem((3 * rank, half), f32),
            vmem((3 * rank, half), f32),
            vmem((nz, 3 * rank, piece), f32),
            vmem((nz, coded_rows, piece), b16),
            vmem((nz - 1, coded_rows, piece), b16),
            vmem((nz, coded_rows, piece), b16),
            vmem((nz, coded_rows, piece), b16),
            vmem((3, 2 * rank, half), b16),
            vmem((nf, thin, cols), f32),
            vmem((nf, rank, wide), f32),
            vmem((nf, thin, cols + 128), b16),
            vmem((nf, rank + 16, wide), b16),
            vmem((nf - 1, thin, cols + 128), b16),
            vmem((nf - 1, rank + 16, wide), b16),
            vmem((nf, thin, cols + 128), b16),
            vmem((wide + 16, rank), b16),
            vmem((nf, wide + 16, rank), b16),
            vmem((nf, wide + 16, rank), b16),
            vmem((nf, 8, 128), f32),
            vmem((nt, 8, 128), f32),
            vmem((early, mq.shape[1]), b16),
            vmem((nf, early, mq.shape[1]), b16),
            vmem((k_early, mk.shape[1]), b16),
            vmem((nf, k_early, mk.shape[1]), b16),
            pltpu.SemaphoreType.DMA((count,)),
            pltpu.SemaphoreType.DMA((count,)),
            pltpu.SemaphoreType.DMA((32,)),
            pltpu.SemaphoreType.DMA((2 * nf,)),
        ],
        compiler_params=pltpu.CompilerParams(
            collective_id=0, has_side_effects=True, vmem_limit_bytes=VMEM_LIMIT
        ),
    )(*args)
    results = list(flushed(results))
    results[6:9] = [r.reshape(-1, r.shape[-1]) for r in results[6:9]]
    return tuple(results)


def per_device(
    normed_inputs,
    query_upstream,
    key_upstream,
    head_outputs,
    branch_upstream,
    query_master,
    key_master,
    branch_master,
    query_basis,
    key_basis,
    branch_basis,
    query_first,
    query_second,
    key_first,
    key_second,
    branch_first,
    branch_second,
):
    exact = lax.Precision.HIGHEST
    row_index = lax.axis_index("fs")
    col_index = lax.axis_index("tp")
    n_rows = lax.axis_size("fs")
    n_cols = lax.axis_size("tp")
    features = normed_inputs.shape[1]
    query_local = query_upstream.shape[1]
    key_local = key_upstream.shape[1]
    rows_in = query_master.shape[0]
    rank = query_basis.shape[1]
    even = n_cols == 2 * n_rows and features * 2 == rows_in and key_local % 128 == 0
    if n_rows == 4 and even and features % 512 == 0 and normed_inputs.shape[0] % 1024 == 0:
        return fused(
            n_rows, n_cols, rows_in // 64 * EARLY_OF_64, normed_inputs, query_upstream, key_upstream,
            head_outputs, branch_upstream, query_master, key_master, branch_master,
            query_basis, key_basis, branch_basis, query_first, query_second,
            key_first, key_second, branch_first, branch_second,
        )

    def own_block(basis):
        return lax.dynamic_slice_in_dim(basis, col_index * features, features, 0)

    block_branch = own_block(branch_basis)
    own_branch = block_branch.astype(jnp.float32)
    lanes = -key_local % 128
    early = rows_in // 32 * 20
    low, branch_low, squares, far = reduced(
        n_rows,
        n_cols,
        early,
        normed_inputs,
        query_upstream,
        jnp.pad(key_upstream, ((0, 0), (0, lanes))),
        head_outputs,
        branch_upstream,
        query_master,
        own_block(query_basis),
        own_block(key_basis),
        block_branch,
    )
    query_low = low[:, :query_local]
    key_low = low[:, query_local : query_local + key_local]
    branch_low = branch_low.reshape(branch_first.shape)
    total = squares[0, 0]
    entries = rank * n_cols * (2 * query_local + key_local)
    rms_value = jnp.sqrt(total / float(entries))
    clip = 1.0 / jnp.maximum(1.0, rms_value / CLIP_RMS)
    q_first, q_second, q_dir = moments(query_first, query_second, query_low, clip)
    k_first, k_second, k_dir = moments(key_first, key_second, key_low, clip)
    b_first, b_second, b_dir = moments(branch_first, branch_second, branch_low, clip)
    step_rows_query = lax.dynamic_slice_in_dim(query_basis, row_index * rows_in, rows_in, 0).astype(
        jnp.float32
    )
    step_rows_key = lax.dynamic_slice_in_dim(key_basis, row_index * rows_in, rows_in, 0).astype(
        jnp.float32
    )
    query_step = jnp.dot(step_rows_query, q_dir, precision=exact)
    key_step = jnp.dot(step_rows_key, k_dir, precision=exact)
    branch_step = jnp.dot(b_dir, own_branch.T, precision=exact)
    query_updated = query_master - LEARN * query_step
    key_updated = key_master - LEARN * key_step
    branch_updated = branch_master - LEARN * branch_step
    query_copy, branch_copy, key_copy = gathered_rows(
        n_rows,
        n_cols,
        query_updated[early:].astype(jnp.bfloat16),
        branch_updated.astype(jnp.bfloat16),
        jnp.pad(key_updated, ((0, 0), (0, lanes))).astype(jnp.bfloat16),
        far,
        query_master,
        query_basis,
        q_dir,
    )
    key_copy = key_copy[:, :key_local]
    return (
        query_step,
        key_step,
        branch_step,
        query_updated,
        key_updated,
        branch_updated,
        query_copy,
        key_copy,
        branch_copy,
        q_first,
        q_second,
        k_first,
        k_second,
        b_first,
        b_second,
    )


def solution(mesh):
    return jax.shard_map(
        per_device,
        mesh=mesh,
        in_specs=(
            P("fs", "tp"),
            P("fs", "tp"),
            P("fs", "tp"),
            P("fs", "tp"),
            P("fs", "tp"),
            P("fs", "tp"),
            P("fs", "tp"),
            P("fs", "tp"),
            P(),
            P(),
            P(),
            P(None, "tp"),
            P(None, "tp"),
            P(None, "tp"),
            P(None, "tp"),
            P("fs", None),
            P("fs", None),
        ),
        out_specs=(
            P("fs", "tp"),
            P("fs", "tp"),
            P("fs", "tp"),
            P("fs", "tp"),
            P("fs", "tp"),
            P("fs", "tp"),
            P(None, "tp"),
            P(None, "tp"),
            P(None, "tp"),
            P(None, "tp"),
            P(None, "tp"),
            P(None, "tp"),
            P(None, "tp"),
            P("fs", None),
            P("fs", None),
        ),
        check_vma=False,
    )
```
